256 devices in a mesh: grp: 2 (over z), sp: 16 (over y, core), tp: 8 (over x).
Axes of the slice: x: 8, y: 8, z: 2, core: 2. Of those that a mesh axis runs over, the one named last changes fastest.
The devices are a block of a 8x8x16 slice.
Arguments:
- residual: bfloat16 [3072, 8, 2048], P(('sp', 'tp'), 'grp'), parts along dimension 1, may hold values from -6 to 6
- query: bfloat16 [3072, 8, 1536], P('sp', 'grp', 'tp'), parts along dimension 1, may hold values from -64 to 64
- latent: bfloat16 [3072, 8, 512], P('sp', 'grp'), parts along dimension 1, may hold values from -6 to 6
- rope_key: bfloat16 [3072, 8, 64], P('sp', 'grp'), parts along dimension 1, may hold values from -8 to 8
- latent_gain: float32 [512], replicated, may hold values from 0.1 to 1.9
- key_up: bfloat16 [512, 1024], P(None, 'tp'), may hold values from -0.25 to 0.25
- value_up: bfloat16 [512, 1024], P(None, 'tp'), may hold values from -0.25 to 0.25
- out_weight: bfloat16 [1024, 2048], P('tp'), may hold values from -0.375 to 0.375
- norm_gain: float32 [2048], replicated, may hold values from 0.1 to 1.9
- group_prob: float32 [3072, 8], P(('sp', 'tp'), 'grp'), parts along dimension 1, may hold values from 0.25 to 1
- pair_logits: float32 [3072, 8, 2], P(('sp', 'tp'), 'grp'), parts along dimension 1, may hold values from -8 to 8
- routes: int32 [3072, 8, 2], P(('sp', 'tp'), 'grp'), parts along dimension 1, may hold values from 0 to 127, all different within a row; in each aligned block of 96 rows (0 to 95, 96 to 191, ..., all dimensions but the last counted through in order) at most 2 rows name the same one
- w_gate: bfloat16 [128, 2048, 768], P(('sp', 'tp')), may hold values from -0.125 to 0.125
- w_up: bfloat16 [128, 2048, 768], P(('sp', 'tp')), may hold values from -0.125 to 0.125
- w_down: bfloat16 [128, 768, 2048], P(('sp', 'tp')), may hold values from -0.4375 to 0.4375
Outputs:
- layer_out: bfloat16 [3072, 8, 2048], P(('sp', 'tp'), 'grp'), parts along dimension 1
The draws below stay inside these ranges and needn't reach their ends.
There are 2 independent parts, one for each index of `grp`. The reference program is written for one: setup_inputs(seed, part) draws one part's arguments, and reference() takes and returns one part's arrays. A program takes and returns all parts, laid end to end along the dimension named above; an argument that names none is the same for every part. Nothing has to cross between parts.
Inputs may be any that keep to these rules, and one draw needn't show every extreme that they name: `routes`: A token's 2 experts differ. Among the tokens of one device (aligned blocks of 96 rows in position-then-sequence order), no expert is named more than 2 times, a bound that some block reaches.
All inputs are finite; a program needn't handle non-finite values.
Results may differ from the reference program's by a relative error of at most 0.013.
Values may be sent and summed in bfloat16 or wider, within the bound.
No kernel may reach another device: no remote copies, remote signals or barrier semaphores. Data moves between devices by JAX's collectives and lax.ppermute only.
A program may use at most 128 MiB of HBM per device.

```python
import math
import jax
import jax.numpy as jnp
import numpy as np
from jax import lax

D = 2048
HEADS = 8
NOPE = 128
ROPE = 64
VDIM = 128
QK = 192
LATENT = 512
FF = 768
TOPK = 2
SEQS = 4
LEN = 3072
ROWS_DEV = 96
EXPERTS = 128
CAP = 2


def draw_rope_key(key, part):
    shape_all = (LEN, SEQS, ROPE)
    drawn = jnp.clip(jax.random.normal(jax.random.fold_in(key, 2), shape_all, jnp.float32), -6.0, 6.0)
    return drawn.astype(jnp.bfloat16)


def draw_query(key, part):
    shape_all = (LEN, SEQS, HEADS * QK)
    drawn = jnp.clip(2.5 * jax.random.normal(jax.random.fold_in(key, 1), shape_all, jnp.float32), -15.0, 15.0)
    return drawn.astype(jnp.bfloat16)


def block_levels(rng, dims, pieces, least, top_value):
    gain, own = 1.0, jax.random.fold_in(rng, 6)
    for position, blocks in pieces:
        steps = jnp.exp(jax.random.uniform(jax.random.fold_in(own, position), (blocks,), jnp.float32, least / len(pieces), top_value / len(pieces)))
        gain = gain * jnp.repeat(steps, dims[position] // blocks).reshape([-1 if axis == position else 1 for axis in range(len(dims))])
    return gain


def assign_block(stream_key, own, number, rows, count, top, bound, skew):
    order = jax.random.permutation(stream_key, count)
    packed, common = load_shares(count, rows * top, bound, skew, True), load_shares(count, rows * top, bound, skew, False)
    places = jnp.arange(count)

    def named(lengths, rotation):
        used = int((lengths > 0).sum())
        fixed = max(1, used // 4)
        moved = fixed + (places - fixed + rotation * (used - fixed)) % max(1, count - fixed)
        return jnp.zeros((count,), jnp.int32).at[order[jnp.where(places < fixed, places, moved)]].set(jnp.asarray(lengths, jnp.int32))

    lengths = jnp.where(number % 4 == 0, named(packed, number // 4), named(common, number - number // 4 - 1))
    mixed = jax.random.permutation(jax.random.fold_in(own, 3), count)
    giver, taker = mixed[0:count // 2 * 2:2], mixed[1:count // 2 * 2:2]
    slack = jnp.minimum(lengths[giver] - 1, bound - lengths[taker]) // 2
    slack = jnp.where((giver == order[0]) | (taker == order[0]) | (lengths[taker] == 0), 0, jnp.maximum(slack, 0))
    moved = jax.random.randint(jax.random.fold_in(own, 4), (count // 2,), 0, 1 << 20) % (slack + 1)
    lengths = lengths.at[giver].add(-moved).at[taker].add(moved)
    members = jnp.searchsorted(jnp.cumsum(lengths), jnp.arange(rows * top), side="right").astype(jnp.int32)
    listing = members.reshape(top, rows).T
    listing = listing[jax.random.permutation(jax.random.fold_in(own, 1), rows)]
    rotation = jax.random.randint(jax.random.fold_in(own, 2), (rows, 1), 0, top)
    return jnp.take_along_axis(listing, (jnp.arange(top)[None, :] + rotation) % top, axis=1)


def load_shares(count, total, reach, slope, full):
    portions = [(1 << 20) // math.isqrt(grade ** slope) + 1 for grade in range(1, count + 1)]
    largest = reach if full else min(reach, max(-(-total // count), total * portions[0] // sum(portions)))
    least = 1 if total - largest >= count - 1 else 0
    given, rest = [largest] + [least] * (count - 1), total - largest - least * (count - 1)
    while rest > 0:
        free = [i for i in range(1, count) if given[i] < largest] or [i for i in range(1, count) if given[i] < reach]
        whole, remaining = sum([portions[i] for i in free]), rest
        for i in free:
            extra = min(reach - given[i], max(1, remaining * portions[i] // whole), rest)
            given[i] = given[i] + extra
            rest = rest - extra
    return np.array(given)


def gaussian(rng, dims, deviation, reach, shards=(), kind=jnp.bfloat16):
    gain = block_levels(rng, dims, shards, -0.22, 0.18) if shards else 1.0
    values = jax.random.normal(rng, dims, jnp.float32) * deviation * gain
    return jnp.minimum(jnp.maximum(values, -reach), reach).astype(kind)


def setup_inputs(seed: int = 0, part: int = 0) -> dict:
    key_list = jax.random.split(jax.random.key(seed), 16)
    part_keys = jax.random.split(jax.random.fold_in(key_list[15], part), 16)
    residual = gaussian(part_keys[0], (LEN, SEQS, D), 1.0, 6.0, ((0, 128),))
    query = draw_query(jax.random.fold_in(jax.random.fold_in(key_list[15], part), 71), part)
    latent = gaussian(part_keys[2], (LEN, SEQS, LATENT), 1.0, 6.0, ((0, 16),))
    rope_key = draw_rope_key(jax.random.fold_in(jax.random.fold_in(key_list[15], part), 71), part)
    latent_gain = jnp.clip(1.0 + 0.18 * jax.random.normal(key_list[4], (LATENT,), jnp.float32), 0.1, 1.9)
    key_up = gaussian(key_list[5], (LATENT, HEADS * NOPE), LATENT ** -0.5, 0.25, ((1, 8),))
    value_up = gaussian(key_list[6], (LATENT, HEADS * VDIM), LATENT ** -0.5, 0.25, ((1, 8),))
    out_weight = gaussian(key_list[7], (HEADS * VDIM, D), (HEADS * VDIM // 4) ** -0.5, 0.375, ((0, 8),))
    norm_gain = jnp.clip(1.0 + 0.18 * jax.random.normal(key_list[8], (D,), jnp.float32), 0.1, 1.9)
    group_prob = jnp.clip(jnp.exp(math.log(1.0) - 1.3862944 * jax.random.uniform(part_keys[9], (LEN, SEQS), jnp.float32) ** block_levels(part_keys[9], (LEN, SEQS), ((0, 128),), -0.2, 0.2)), 0.25, 1.0)
    pair_logits = gaussian(part_keys[10], (LEN, SEQS, TOPK), 1.5, 8.0, ((0, 128),), jnp.float32)
    routes_keys = jax.random.split(jax.random.fold_in(part_keys[11], 1), LEN * SEQS // ROWS_DEV)
    routes_turns = jax.random.permutation(jax.random.fold_in(part_keys[11], 3), LEN * SEQS // ROWS_DEV)
    routes = jax.vmap(lambda own, number: assign_block(jax.random.fold_in(part_keys[11], 2), own, number, ROWS_DEV, EXPERTS, TOPK, CAP, 1))(routes_keys, routes_turns).reshape((LEN, SEQS, TOPK))
    w_gate = gaussian(key_list[12], (EXPERTS, D, FF), D ** -0.5, 0.125, ((0, 128),))
    w_up = gaussian(key_list[13], (EXPERTS, D, FF), D ** -0.5, 0.125, ((0, 128),))
    w_down = gaussian(key_list[14], (EXPERTS, FF, D), (FF // 4) ** -0.5, 0.4375, ((0, 128),))
    return {"residual": residual, "query": query, "latent": latent, "rope_key": rope_key, "latent_gain": latent_gain, "key_up": key_up, "value_up": value_up, "out_weight": out_weight, "norm_gain": norm_gain, "group_prob": group_prob, "pair_logits": pair_logits, "routes": routes, "w_gate": w_gate, "w_up": w_up, "w_down": w_down}


epsilon = 1e-06
rotary_base = 10000.0

def rotate(values, positions):
    halfway = values.shape[-1] // 2
    inverse = rotary_base ** (-jnp.arange(halfway, dtype=jnp.float32) / halfway)
    angles = positions.astype(jnp.float32)[:, None] * inverse[None, :]
    angles = angles.reshape((angles.shape[0],) + (1,) * (values.ndim - 2) + (halfway,))
    cosine_values = jnp.cos(angles)
    sine_values = jnp.sin(angles)
    first_half = values[..., :halfway]
    second_half = values[..., halfway:]
    return jnp.concatenate([first_half * cosine_values - second_half * sine_values, second_half * cosine_values + first_half * sine_values], axis=-1)

def rms_scale(values, gain_values):
    return values * lax.rsqrt(lax.optimization_barrier(jnp.mean(values * values, axis=-1, keepdims=True)) + epsilon) * gain_values

def expand(latent_rows, latent_gain, key_up, value_up):
    normed = rms_scale(latent_rows.astype(jnp.float32), latent_gain).astype(jnp.bfloat16)
    keys_nope = jnp.dot(normed, key_up, preferred_element_type=jnp.float32).astype(jnp.bfloat16)
    values = jnp.dot(normed, value_up, preferred_element_type=jnp.float32).astype(jnp.bfloat16)
    lead = latent_rows.shape[:2]
    return (keys_nope.reshape(lead + (key_up.shape[1] // NOPE, NOPE)), values.reshape(lead + (value_up.shape[1] // VDIM, VDIM)))

def reference(residual, query, latent, rope_key, latent_gain, key_up, value_up, out_weight, norm_gain, group_prob, pair_logits, routes, w_gate, w_up, w_down):
    positions = jnp.arange(LEN, dtype=jnp.int32)
    key_nope, value_rows = expand(latent, latent_gain, key_up, value_up)
    key_rot = rotate(rope_key.astype(jnp.float32), positions).astype(jnp.bfloat16)
    split_query = query.reshape(LEN, SEQS, HEADS, QK)
    query_nope = split_query[..., :NOPE]
    query_rot = rotate(split_query[..., NOPE:].astype(jnp.float32), positions).astype(jnp.bfloat16)

    def attend(inputs):
        head_nope, head_rot, head_keys, head_values = inputs
        scores = jnp.einsum('qsd,ksd->sqk', head_nope.astype(jnp.float32), head_keys.astype(jnp.float32))
        scores = scores + jnp.einsum('qsd,ksd->sqk', head_rot.astype(jnp.float32), key_rot.astype(jnp.float32))
        scores = scores * QK ** (-0.5)
        highest = lax.optimization_barrier(jnp.max(scores, axis=-1, keepdims=True))
        weights = jnp.exp(scores - highest)
        totals = lax.optimization_barrier(jnp.sum(weights, axis=-1))
        rounded = lax.optimization_barrier(weights.astype(jnp.bfloat16)).astype(jnp.float32)
        mixed = jnp.einsum('sqk,ksd->sqd', rounded, head_values.astype(jnp.float32))
        return (mixed / totals[..., None]).astype(jnp.bfloat16)
    heads_out = lax.map(attend, (jnp.moveaxis(query_nope, 2, 0), jnp.moveaxis(query_rot, 2, 0), jnp.moveaxis(key_nope, 2, 0), jnp.moveaxis(value_rows, 2, 0)))
    row_total = LEN * SEQS
    attended = jnp.transpose(heads_out, (2, 1, 0, 3)).reshape(row_total, HEADS * VDIM)
    projected = jnp.dot(attended, out_weight, preferred_element_type=jnp.float32)
    stream = (residual.reshape(row_total, D).astype(jnp.float32) + projected).astype(jnp.bfloat16)
    normed = rms_scale(stream.astype(jnp.float32), norm_gain).astype(jnp.bfloat16)
    mixing = jax.nn.softmax(pair_logits.reshape(row_total, TOPK), axis=-1) * group_prob.reshape(row_total, 1)
    blocks = row_total // ROWS_DEV
    chosen = routes.reshape(blocks, ROWS_DEV * TOPK).astype(jnp.int32)
    one_hot = (chosen[..., None] == jnp.arange(EXPERTS, dtype=jnp.int32)).astype(jnp.int32)
    before = jnp.cumsum(one_hot, axis=1) - one_hot
    slot_index = lax.optimization_barrier(jnp.sum(before * one_hot, axis=-1)).astype(jnp.int32)
    column = (jnp.arange(blocks, dtype=jnp.int32)[:, None] * CAP + slot_index).astype(jnp.int32)
    source_row = (jnp.arange(row_total * TOPK, dtype=jnp.int32).reshape(blocks, ROWS_DEV * TOPK) // TOPK).astype(jnp.int32)
    slot_table = jnp.full((EXPERTS, blocks * CAP), row_total, jnp.int32).at[chosen, column].set(source_row)
    padded = jnp.concatenate([normed, jnp.zeros((1, D), jnp.bfloat16)], axis=0)

    def serve_rows(expert_inputs):
        row_numbers, gate_weight, up_weight, down_weight = expert_inputs
        gathered = padded[row_numbers]
        gate_pre = jnp.dot(gathered, gate_weight, preferred_element_type=jnp.float32)
        upward = jnp.dot(gathered, up_weight, preferred_element_type=jnp.float32)
        hidden = (jax.nn.silu(gate_pre) * upward).astype(jnp.bfloat16)
        return jnp.dot(hidden, down_weight, preferred_element_type=jnp.float32).astype(jnp.bfloat16)
    served = lax.map(serve_rows, (slot_table, w_gate, w_up, w_down))
    results = served[chosen, column].reshape(row_total, TOPK, D)
    combined = stream.astype(jnp.float32) + lax.optimization_barrier(jnp.sum(results.astype(jnp.float32) * mixing[..., None], axis=1))
    return combined.astype(jnp.bfloat16).reshape(LEN, SEQS, D)
```

```python
import jax
import jax.numpy as jnp
import numpy as np
from jax import lax
from jax.experimental import pallas as pl
from jax.experimental.pallas import tpu as pltpu
from jax.sharding import Mesh, PartitionSpec as P

D = 2048
NOPE = 128
ROPE = 64
VDIM = 128
QK = 192
SEQS = 4
CHIPS = 8
LANE = 256
BANDS = D // LANE

epsilon = 1e-06
rotary_base = 10000.0
score_scale = QK ** (-0.5) * 1.4426950408889634

Y = ("half", "quad")
ALL = ("half", "quad", "core", "tp")


def rotate(values, positions):
    halfway = values.shape[-1] // 2
    inverse = rotary_base ** (-jnp.arange(halfway, dtype=jnp.float32) / halfway)
    angles = positions.astype(jnp.float32)[:, None] * inverse[None, :]
    angles = angles.reshape((1, angles.shape[0], halfway))
    cosine_values = jnp.cos(angles)
    sine_values = jnp.sin(angles)
    first_half = values[..., :halfway]
    second_half = values[..., halfway:]
    return jnp.concatenate(
        [
            first_half * cosine_values - second_half * sine_values,
            second_half * cosine_values + first_half * sine_values,
        ],
        axis=-1,
    )


def dot(a, b):
    return lax.dot_general(a, b, (((1,), (0,)), ((), ())), preferred_element_type=jnp.float32)


def packing(inverse):
    i = lax.broadcasted_iota(jnp.int32, (256, 256), 1 if inverse else 0)
    k = lax.broadcasted_iota(jnp.int32, (256, 256), 0 if inverse else 1)
    d, r = i // 16, i % 16
    return (k == (r // 2) * 32 + (r % 2) * 16 + d).astype(jnp.bfloat16)


def pack_rows(rows_ref, out_ref, perm):
    for b in range(8):
        stack = []
        for j in range(BANDS):
            for slot in range(2):
                lo = slot * 128 + b * 16
                stack.append(rows_ref[lo : lo + 16, j * LANE : (j + 1) * LANE])
        out_ref[b * 256 : (b + 1) * 256, :] = dot(perm, jnp.concatenate(stack, axis=0)).astype(
            jnp.bfloat16
        )


def unpack_rows(in_ref, rows_ref, perm):
    for b in range(8):
        block = dot(perm, in_ref[b * 256 : (b + 1) * 256, :]).astype(jnp.bfloat16)
        for j in range(BANDS):
            for slot in range(2):
                lo = slot * 128 + b * 16
                at = j * 32 + slot * 16
                rows_ref[lo : lo + 16, j * LANE : (j + 1) * LANE] = block[at : at + 16, :]


def places(meta):
    rows = meta.shape[0]
    expert = lax.broadcasted_iota(jnp.int32, (rows, 128), 1).astype(jnp.float32)
    first = (meta[:, 0:1] == expert).astype(jnp.float32)
    second = (meta[:, 1:2] == expert).astype(jnp.float32)
    earlier = (
        lax.broadcasted_iota(jnp.int32, (rows, rows), 0)
        > lax.broadcasted_iota(jnp.int32, (rows, rows), 1)
    ).astype(jnp.bfloat16)
    before = dot(earlier, (first + second).astype(jnp.bfloat16))
    return first, second, before


def attention_body(q_ref, a_ref, b_ref, o_ref, keys, values):
    for i in range(16):
        src = a_ref if i < 8 else b_ref
        j = i % 8
        lo, hi = i * 96, 1536 + i * 96
        keys[lo : lo + 96, 0:128] = src[j, 0:96, :]
        keys[hi : hi + 96, 0:128] = src[j, 96:192, :]
        values[lo : lo + 96, :] = src[j, 192:288, :]
        values[hi : hi + 96, :] = src[j, 288:384, :]
        rot = src[j, 384:480, :]
        keys[lo : lo + 96, 128:256] = rot
        keys[hi : hi + 96, 128:256] = pltpu.roll(rot.astype(jnp.float32), 64, 1).astype(
            jnp.bfloat16
        )
    for n in range(3):
        q = q_ref[n * 256 : (n + 1) * 256, :]
        scores = lax.dot_general(
            q, keys[...], (((1,), (1,)), ((), ())), preferred_element_type=jnp.float32
        )
        highest = jnp.max(scores, axis=-1, keepdims=True)
        weights = jnp.exp2((scores - highest) * score_scale)
        totals = jnp.sum(weights, axis=-1, keepdims=True)
        out = dot(weights.astype(jnp.bfloat16), values[...])
        o_ref[n * 256 : (n + 1) * 256, :] = (out / totals).astype(jnp.bfloat16)


def project_body(
    at_ref, att_ref, own_ref, other_ref, res_ref, gain_ref, meta_ref, stream_ref, out_ref, lhs, acc, rows
):
    tp, core = at_ref[0], at_ref[1]
    for k in range(8):
        lhs[:, k * 128 : (k + 1) * 128] = att_ref[(tp + 8 - k) % 8]
    acc[:, pl.ds(pl.multiple_of(core * 1024, 1024), 1024)] = dot(lhs[...], own_ref[...])
    acc[:, pl.ds(pl.multiple_of((1 - core) * 1024, 1024), 1024)] = dot(lhs[...], other_ref[...])
    stream = (res_ref[...].astype(jnp.float32) + acc[...]).astype(jnp.bfloat16)
    stream_ref[...] = stream
    wide = stream.astype(jnp.float32)
    normed = (
        wide * lax.rsqrt(jnp.mean(wide * wide, axis=-1, keepdims=True) + epsilon) * gain_ref[...]
    ).astype(jnp.bfloat16)
    first, second, before = places(meta_ref[...])
    both = first + second
    for slot in range(2):
        pick = (both * (before == slot).astype(jnp.float32)).T.astype(jnp.bfloat16)
        rows[slot * 128 : (slot + 1) * 128, :] = dot(pick, normed).astype(jnp.bfloat16)
    pack_rows(rows, out_ref, packing(False))


def expert_body(in_ref, gate_ref, up_ref, down_ref, out_ref, rows, acc):
    step = pl.program_id(0)

    @pl.when(step == 0)
    def _():
        unpack_rows(in_ref, rows, packing(True))

    x = rows[...]
    gate = dot(x, gate_ref[...])
    up = dot(x, up_ref[...])
    hidden = (gate / (1.0 + jnp.exp(-gate)) * up).astype(jnp.bfloat16)
    part = dot(hidden, down_ref[...])

    @pl.when(step == 0)
    def _():
        acc[...] = part

    @pl.when(step > 0)
    def _():
        acc[...] += part

    @pl.when(step == pl.num_programs(0) - 1)
    def _():
        rows[...] = acc[...].astype(jnp.bfloat16)
        pack_rows(rows, out_ref, packing(False))


def combine_body(in_ref, stream_ref, meta_ref, out_ref, rows):
    unpack_rows(in_ref, rows, packing(True))
    meta = meta_ref[...]
    first, second, before = places(meta)
    logits = meta[:, 2:4]
    weights = jnp.exp(logits - jnp.max(logits, axis=-1, keepdims=True))
    mixing = weights / jnp.sum(weights, axis=-1, keepdims=True) * meta[:, 4:5]
    slots = [(before == slot).astype(jnp.float32) for slot in range(2)]
    total = stream_ref[...].astype(jnp.float32)
    r = rows[...]
    added = None
    for k, hot in enumerate((first, second)):
        pick = jnp.concatenate([hot * slots[0], hot * slots[1]], axis=-1).astype(jnp.bfloat16)
        term = dot(pick, r) * mixing[:, k : k + 1]
        added = term if added is None else added + term
    out_ref[...] = (total + added).astype(jnp.bfloat16)


def vmem(*shape):
    return pltpu.VMEM(shape, jnp.bfloat16)


def params():
    return pltpu.CompilerParams(vmem_limit_bytes=56 * 1024 * 1024)


VM = pl.BlockSpec(memory_space=pltpu.VMEM)
SM = pl.BlockSpec(memory_space=pltpu.SMEM)


def shards(
    residual,
    query,
    latent,
    rope_key,
    latent_gain,
    key_up,
    value_up,
    out_weight,
    norm_gain,
    group_prob,
    pair_logits,
    routes,
    w_gate,
    w_up,
    w_down,
):
    tp = lax.axis_index("tp")
    core = lax.axis_index("core")
    block = query.shape[0]
    rows = residual.shape[0] * SEQS
    tp_size = lax.axis_size("tp")
    at = jnp.stack([tp, core]).astype(jnp.int32)

    half_cols = D // 2
    own = lax.dynamic_slice(out_weight, (0, core * half_cols), (out_weight.shape[0], half_cols))
    pieces = [own]
    for k in range(1, tp_size):
        pieces.append(lax.ppermute(own, "tp", [(i, (i + k) % tp_size) for i in range(tp_size)]))
    own_cols = jnp.concatenate(pieces, axis=0)
    other_cols = lax.ppermute(own_cols, "core", [(0, 1), (1, 0)])

    spot = (lax.axis_index("half") * 4 + lax.axis_index("quad")) * 2 + core
    positions = spot * block + jnp.arange(block, dtype=jnp.int32)
    q = jnp.swapaxes(query, 0, 1)
    q_rot = rotate(q[..., NOPE:].astype(jnp.float32), positions).astype(jnp.bfloat16)
    q = jnp.concatenate([q[..., :NOPE], q_rot, jnp.zeros_like(q_rot)], axis=-1)
    q = lax.all_to_all(q, "quad", split_axis=0, concat_axis=0, tiled=True)

    lat = jnp.swapaxes(latent, 0, 1).astype(jnp.float32)
    lat = (
        lat * lax.rsqrt(jnp.mean(lat * lat, axis=-1, keepdims=True) + epsilon) * latent_gain
    ).astype(jnp.bfloat16)
    keys = jnp.einsum("spd,dc->spc", lat, key_up, preferred_element_type=jnp.float32)
    vals = jnp.einsum("spd,dc->spc", lat, value_up, preferred_element_type=jnp.float32)
    rot = rotate(jnp.swapaxes(rope_key, 0, 1).astype(jnp.float32), positions)
    rot = jnp.concatenate([rot[:, : block // 2], rot[:, block // 2 :]], axis=-1)
    kv = jnp.concatenate([keys, vals, rot], axis=1).astype(jnp.bfloat16)
    kv = jnp.concatenate([kv, kv], axis=0)
    near = lax.all_to_all(kv, Y, split_axis=0, concat_axis=0, tiled=True)
    far = lax.ppermute(near, "core", [(0, 1), (1, 0)])

    attended = pl.pallas_call(
        attention_body,
        out_shape=jax.ShapeDtypeStruct((4 * block, VDIM), jnp.bfloat16),
        in_specs=[VM, VM, VM],
        out_specs=VM,
        scratch_shapes=[vmem(16 * block, 256), vmem(16 * block, VDIM)],
        compiler_params=params(),
        name="attention",
    )(q.reshape(4 * block, 256), near, far)
    attended = attended.reshape(4 * tp_size, block // tp_size, VDIM)
    attended = lax.all_to_all(attended, ("quad", "tp"), split_axis=0, concat_axis=0, tiled=True)
    attended = attended.reshape(SEQS, tp_size, block // tp_size, VDIM)
    attended = jnp.swapaxes(attended, 0, 1).reshape(tp_size, rows, VDIM)

    res = jnp.swapaxes(residual, 0, 1).reshape(rows, D)
    meta = jnp.concatenate(
        [routes.astype(jnp.float32), pair_logits, group_prob[..., None]], axis=-1
    )
    meta = jnp.swapaxes(meta, 0, 1).reshape(rows, 5)
    stream, outgoing = pl.pallas_call(
        project_body,
        out_shape=(
            jax.ShapeDtypeStruct((rows, D), jnp.bfloat16),
            jax.ShapeDtypeStruct((2048, LANE), jnp.bfloat16),
        ),
        in_specs=[SM] + [VM] * 6,
        out_specs=(VM, VM),
        scratch_shapes=[vmem(rows, 1024), pltpu.VMEM((rows, D), jnp.float32), vmem(256, D)],
        compiler_params=params(),
        name="project",
    )(at, attended, own_cols, other_cols, res, norm_gain.reshape(1, D), meta)

    def exchange(x):
        x = x.reshape(128, 16, LANE)
        return lax.all_to_all(x, ALL, split_axis=0, concat_axis=0, tiled=True).reshape(2048, LANE)

    arrived = exchange(outgoing)
    hidden = w_gate.shape[2]
    step = 256
    served = pl.pallas_call(
        expert_body,
        out_shape=jax.ShapeDtypeStruct((2048, LANE), jnp.bfloat16),
        grid=(hidden // step,),
        in_specs=[
            pl.BlockSpec((2048, LANE), lambda i: (0, 0)),
            pl.BlockSpec((D, step), lambda i: (0, i)),
            pl.BlockSpec((D, step), lambda i: (0, i)),
            pl.BlockSpec((step, D), lambda i: (i, 0)),
        ],
        out_specs=pl.BlockSpec((2048, LANE), lambda i: (0, 0)),
        scratch_shapes=[vmem(256, D), pltpu.VMEM((256, D), jnp.float32)],
        compiler_params=params(),
        name="experts",
    )(arrived, w_gate[0], w_up[0], w_down[0])
    returned = exchange(served)
    combined = pl.pallas_call(
        combine_body,
        out_shape=jax.ShapeDtypeStruct((rows, D), jnp.bfloat16),
        in_specs=[VM] * 3,
        out_specs=VM,
        scratch_shapes=[vmem(256, D)],
        compiler_params=params(),
        name="combine",
    )(returned, stream, meta)
    return jnp.swapaxes(combined.reshape(SEQS, rows // SEQS, D), 0, 1)


def solution(mesh):
    shape = mesh.shape
    devices = np.asarray(mesh.devices).reshape(
        shape["grp"], 2, 4, shape["sp"] // 8, shape["tp"]
    )
    fine = Mesh(devices, ("grp", "half", "quad", "core", "tp"))
    sp = ("half", "quad", "core")
    both = ("half", "quad", "core", "tp")
    placed = (
        P(both, "grp", None),
        P(sp, "grp", "tp"),
        P(sp, "grp", None),
        P(sp, "grp", None),
        P(),
        P(None, "tp"),
        P(None, "tp"),
        P("tp", None),
        P(),
        P(both, "grp"),
        P(both, "grp", None),
        P(both, "grp", None),
        P(both, None, None),
        P(both, None, None),
        P(both, None, None),
    )
    return jax.shard_map(
        shards, mesh=fine, in_specs=placed, out_specs=P(both, "grp", None), check_vma=False
    )
```

```python
import jax
import jax.numpy as jnp
import numpy as np
from jax import lax
from jax.experimental import pallas as pl
from jax.experimental.pallas import tpu as pltpu
from jax.sharding import Mesh, PartitionSpec as P


D = 2048
NOPE = 128
VDIM = 128
QK = 192
SEQS = 4
LANE = 256
BANDS = D // LANE

epsilon = 1e-06
rotary_base = 10000.0
score_scale = QK ** (-0.5) * 1.4426950408889634

Y = ("half", "quad")
ALL = ("half", "quad", "core", "tp")


def rotate(values, positions):
    halfway = values.shape[-1] // 2
    inverse = rotary_base ** (-jnp.arange(halfway, dtype=jnp.float32) / halfway)
    angles = positions.astype(jnp.float32)[:, None] * inverse[None, :]
    angles = angles.reshape((1, angles.shape[0], halfway))
    cosine_values = jnp.cos(angles)
    sine_values = jnp.sin(angles)
    first_half = values[..., :halfway]
    second_half = values[..., halfway:]
    return jnp.concatenate(
        [
            first_half * cosine_values - second_half * sine_values,
            second_half * cosine_values + first_half * sine_values,
        ],
        axis=-1,
    )


def shift(x, axis, by, size):
    if by == 0:
        return x
    return lax.ppermute(x, axis, [(i, (i + by) % size) for i in range(size)])


def swap(x):
    return lax.ppermute(x, "core", [(0, 1), (1, 0)])


def spread(x, by, size):
    pairs = []
    for i in range(size):
        pairs.append((i, (i + by) % size))
        pairs.append((size + i, size + (i - by) % size))
    return lax.ppermute(x, ("core", "tp"), pairs)


def dot(a, b):
    return lax.dot_general(a, b, (((1,), (0,)), ((), ())), preferred_element_type=jnp.float32)


def packing(inverse):
    i = lax.broadcasted_iota(jnp.int32, (256, 256), 1 if inverse else 0)
    k = lax.broadcasted_iota(jnp.int32, (256, 256), 0 if inverse else 1)
    d, r = i // 16, i % 16
    return (k == (r // 2) * 32 + (r % 2) * 16 + d).astype(jnp.bfloat16)


def pack_rows(rows_ref, out_ref, perm):
    for b in range(8):
        stack = []
        for j in range(BANDS):
            for slot in range(2):
                lo = slot * 128 + b * 16
                stack.append(rows_ref[lo : lo + 16, j * LANE : (j + 1) * LANE])
        out_ref[b * 256 : (b + 1) * 256, :] = dot(perm, jnp.concatenate(stack, axis=0)).astype(
            jnp.bfloat16
        )


def unpack_rows(in_ref, rows_ref, perm):
    for b in range(8):
        block = dot(perm, in_ref[b * 256 : (b + 1) * 256, :]).astype(jnp.bfloat16)
        for j in range(BANDS):
            for slot in range(2):
                lo = slot * 128 + b * 16
                at = j * 32 + slot * 16
                rows_ref[lo : lo + 16, j * LANE : (j + 1) * LANE] = block[at : at + 16, :]


def places(meta):
    rows = meta.shape[0]
    expert = lax.broadcasted_iota(jnp.int32, (rows, 128), 1).astype(jnp.float32)
    first = (meta[:, 0:1] == expert).astype(jnp.float32)
    second = (meta[:, 1:2] == expert).astype(jnp.float32)
    earlier = (
        lax.broadcasted_iota(jnp.int32, (rows, rows), 0)
        > lax.broadcasted_iota(jnp.int32, (rows, rows), 1)
    ).astype(jnp.bfloat16)
    before = dot(earlier, (first + second).astype(jnp.bfloat16))
    return first, second, before


def attention_body(at_ref, q_ref, a_ref, b_ref, o_ref, keys, values):
    quad = at_ref[2]
    for i in range(16):
        src = a_ref if i < 8 else b_ref
        j = i % 8
        lo, hi = i * 96, 1536 + i * 96
        keys[lo : lo + 96, 0:128] = src[j, 0:96, :]
        keys[hi : hi + 96, 0:128] = src[j, 96:192, :]
        values[lo : lo + 96, :] = src[j, 192:288, :]
        values[hi : hi + 96, :] = src[j, 288:384, :]
        rot = src[j, 384:480, :]
        keys[lo : lo + 96, 128:256] = rot
        keys[hi : hi + 96, 128:256] = pltpu.roll(rot.astype(jnp.float32), 64, 1).astype(
            jnp.bfloat16
        )
    for n in range(4):
        q = q_ref[n * 192 : (n + 1) * 192, :]
        scores = lax.dot_general(
            q, keys[...], (((1,), (1,)), ((), ())), preferred_element_type=jnp.float32
        )
        highest = jnp.max(scores, axis=-1, keepdims=True)
        weights = jnp.exp2((scores - highest) * score_scale)
        totals = jnp.sum(weights, axis=-1, keepdims=True)
        out = dot(weights.astype(jnp.bfloat16), values[...])
        o_ref[(quad + 4 - n) % 4] = (out / totals).astype(jnp.bfloat16)


def project_body(
    at_ref,
    att_ref,
    w0,
    w1,
    w2,
    w3,
    s1,
    s2,
    s3,
    w4,
    s4,
    res_ref,
    gain_ref,
    meta_ref,
    stream_ref,
    out_ref,
    rows,
):
    tp, core = at_ref[0], at_ref[1]
    turn = 1 - 2 * core
    projected = dot(att_ref[tp], w0[...])
    for k, w_ref in ((1, w1), (2, w2), (3, w3), (-1, s1), (-2, s2), (-3, s3)):
        projected += dot(att_ref[(tp + 8 - turn * k) % 8], w_ref[...])
    last = att_ref[(tp + 4) % 8]
    turned = pltpu.roll(last.astype(jnp.float32), 64, 1).astype(jnp.bfloat16)
    last = jnp.where(core == 0, last, turned)
    projected += dot(last[:, :64], w4[...]) + dot(last[:, 64:], s4[...])
    stream = (res_ref[...].astype(jnp.float32) + projected).astype(jnp.bfloat16)
    stream_ref[...] = stream
    wide = stream.astype(jnp.float32)
    normed = (
        wide * lax.rsqrt(jnp.mean(wide * wide, axis=-1, keepdims=True) + epsilon) * gain_ref[...]
    ).astype(jnp.bfloat16)
    first, second, before = places(meta_ref[...])
    both = first + second
    for slot in range(2):
        pick = (both * (before == slot).astype(jnp.float32)).T.astype(jnp.bfloat16)
        rows[slot * 128 : (slot + 1) * 128, :] = dot(pick, normed).astype(jnp.bfloat16)
    pack_rows(rows, out_ref, packing(False))


def expert_body(in_ref, gate_ref, up_ref, down_ref, out_ref, rows, acc):
    step = pl.program_id(0)

    @pl.when(step == 0)
    def _():
        unpack_rows(in_ref, rows, packing(True))

    x = rows[...]
    gate = dot(x, gate_ref[...])
    up = dot(x, up_ref[...])
    hidden = (gate / (1.0 + jnp.exp(-gate)) * up).astype(jnp.bfloat16)
    part = dot(hidden, down_ref[...])

    @pl.when(step == 0)
    def _():
        acc[...] = part

    @pl.when(step > 0)
    def _():
        acc[...] += part

    @pl.when(step == pl.num_programs(0) - 1)
    def _():
        rows[...] = acc[...].astype(jnp.bfloat16)
        pack_rows(rows, out_ref, packing(False))


def combine_body(in_ref, stream_ref, meta_ref, out_ref, rows):
    unpack_rows(in_ref, rows, packing(True))
    meta = meta_ref[...]
    first, second, before = places(meta)
    logits = meta[:, 2:4]
    weights = jnp.exp(logits - jnp.max(logits, axis=-1, keepdims=True))
    mixing = weights / jnp.sum(weights, axis=-1, keepdims=True) * meta[:, 4:5]
    slots = [(before == slot).astype(jnp.float32) for slot in range(2)]
    total = stream_ref[...].astype(jnp.float32)
    r = rows[...]
    added = None
    for k, hot in enumerate((first, second)):
        pick = jnp.concatenate([hot * slots[0], hot * slots[1]], axis=-1).astype(jnp.bfloat16)
        term = dot(pick, r) * mixing[:, k : k + 1]
        added = term if added is None else added + term
    out_ref[...] = (total + added).astype(jnp.bfloat16)


def vmem(*shape):
    return pltpu.VMEM(shape, jnp.bfloat16)


def params():
    return pltpu.CompilerParams(vmem_limit_bytes=56 * 1024 * 1024)


def kernel_call(body, **options):
    return pl.pallas_call(body, compiler_params=params(), **options)


VM = pl.BlockSpec(memory_space=pltpu.VMEM)
SM = pl.BlockSpec(memory_space=pltpu.SMEM)


def layer(
    residual,
    query,
    latent,
    rope_key,
    latent_gain,
    key_up,
    value_up,
    out_weight,
    norm_gain,
    group_prob,
    pair_logits,
    routes,
    w_gate,
    w_up,
    w_down,
):
    tp = lax.axis_index("tp")
    core = lax.axis_index("core")
    block = query.shape[0]
    rows = residual.shape[0] * SEQS
    tp_size = lax.axis_size("tp")
    quad = lax.axis_index("quad")
    at = jnp.stack([tp, core, quad]).astype(jnp.int32)

    spot = (lax.axis_index("half") * 4 + lax.axis_index("quad")) * 2 + core
    positions = spot * block + jnp.arange(block, dtype=jnp.int32)
    q = jnp.swapaxes(query, 0, 1)
    q_rot = rotate(q[..., NOPE:].astype(jnp.float32), positions).astype(jnp.bfloat16)
    q = jnp.concatenate([q[..., :NOPE], q_rot, jnp.zeros_like(q_rot)], axis=-1)
    queries = []
    for k in range(4):
        piece = lax.dynamic_index_in_dim(q, (quad + k) % 4, 0, keepdims=False)
        queries.append(shift(piece, "quad", k, 4))
    queries = jnp.concatenate(queries, axis=0)

    lat = jnp.swapaxes(latent, 0, 1).astype(jnp.float32)
    lat = (
        lat * lax.rsqrt(jnp.mean(lat * lat, axis=-1, keepdims=True) + epsilon) * latent_gain
    ).astype(jnp.bfloat16)
    keys = jnp.einsum("spd,dc->spc", lat, key_up, preferred_element_type=jnp.float32)
    vals = jnp.einsum("spd,dc->spc", lat, value_up, preferred_element_type=jnp.float32)
    rot = rotate(jnp.swapaxes(rope_key, 0, 1).astype(jnp.float32), positions)
    rot = jnp.concatenate([rot[:, : block // 2], rot[:, block // 2 :]], axis=-1)
    kv = jnp.concatenate([keys, vals, rot], axis=1).astype(jnp.bfloat16)
    kv = jnp.concatenate([kv, kv], axis=0)
    half_rows = out_weight.shape[0] // 2
    one, two = spread(out_weight, 1, tp_size), spread(out_weight, 2, tp_size)
    three = spread(two, 1, tp_size)
    part = lax.dynamic_slice(two, (core * half_rows, 0), (half_rows, D))
    four = spread(part, 2, tp_size)
    weights = [out_weight, one, two, three, swap(one), swap(two)]
    weights += [swap(three), four, swap(four)]

    near = lax.all_to_all(kv, Y, split_axis=0, concat_axis=0, tiled=True)
    far = swap(near)

    attended = kernel_call(
        attention_body,
        out_shape=jax.ShapeDtypeStruct((4, block, VDIM), jnp.bfloat16),
        in_specs=[SM] + [VM] * 3,
        out_specs=VM,
        scratch_shapes=[vmem(16 * block, 256), vmem(16 * block, VDIM)],
    )(at, queries, near, far)
    attended = attended.reshape(4 * tp_size, block // tp_size, VDIM)
    attended = lax.all_to_all(attended, ("quad", "tp"), split_axis=0, concat_axis=0, tiled=True)
    attended = attended.reshape(SEQS, tp_size, block // tp_size, VDIM)
    attended = jnp.swapaxes(attended, 0, 1).reshape(tp_size, rows, VDIM)

    res = jnp.swapaxes(residual, 0, 1).reshape(rows, D)
    meta = jnp.concatenate(
        [routes.astype(jnp.float32), pair_logits, group_prob[..., None]], axis=-1
    )
    meta = jnp.swapaxes(meta, 0, 1).reshape(rows, 5)
    stream, outgoing = pl.pallas_call(
        project_body,
        out_shape=(
            jax.ShapeDtypeStruct((rows, D), jnp.bfloat16),
            jax.ShapeDtypeStruct((2048, LANE), jnp.bfloat16),
        ),
        in_specs=[SM] + [VM] * 13,
        out_specs=(VM, VM),
        scratch_shapes=[vmem(256, D)],
        compiler_params=params(),
        name="project",
    )(at, attended, *weights, res, norm_gain.reshape(1, D), meta)

    def exchange(x):
        x = x.reshape(128, 16, LANE)
        return lax.all_to_all(x, ALL, split_axis=0, concat_axis=0, tiled=True).reshape(2048, LANE)

    arrived = exchange(outgoing)
    hidden = w_gate.shape[2]
    step = 256
    served = pl.pallas_call(
        expert_body,
        out_shape=jax.ShapeDtypeStruct((2048, LANE), jnp.bfloat16),
        grid=(hidden // step,),
        in_specs=[
            pl.BlockSpec((2048, LANE), lambda i: (0, 0)),
            pl.BlockSpec((D, step), lambda i: (0, i)),
            pl.BlockSpec((D, step), lambda i: (0, i)),
            pl.BlockSpec((step, D), lambda i: (i, 0)),
        ],
        out_specs=pl.BlockSpec((2048, LANE), lambda i: (0, 0)),
        scratch_shapes=[vmem(256, D), pltpu.VMEM((256, D), jnp.float32)],
        compiler_params=params(),
        name="experts",
    )(arrived, w_gate[0], w_up[0], w_down[0])
    returned = exchange(served)
    combined = pl.pallas_call(
        combine_body,
        out_shape=jax.ShapeDtypeStruct((rows, D), jnp.bfloat16),
        in_specs=[VM] * 3,
        out_specs=VM,
        scratch_shapes=[vmem(256, D)],
        compiler_params=params(),
        name="combine",
    )(returned, stream, meta)
    return jnp.swapaxes(combined.reshape(SEQS, rows // SEQS, D), 0, 1)


def solution(mesh):
    shape = mesh.shape
    devices = np.asarray(mesh.devices).reshape(
        shape["grp"], 2, 4, shape["sp"] // 8, shape["tp"]
    )
    fine = Mesh(devices, ("grp", "half", "quad", "core", "tp"))
    sp = ("half", "quad", "core")
    both = ("half", "quad", "core", "tp")
    placed = (
        P(both, "grp", None),
        P(sp, "grp", "tp"),
        P(sp, "grp", None),
        P(sp, "grp", None),
        P(),
        P(None, "tp"),
        P(None, "tp"),
        P("tp", None),
        P(),
        P(both, "grp"),
        P(both, "grp", None),
        P(both, "grp", None),
        P(both, None, None),
        P(both, None, None),
        P(both, None, None),
    )
    return jax.shard_map(
        layer, mesh=fine, in_specs=placed, out_specs=P(both, "grp", None), check_vma=False
    )
```

```python
import jax
import jax.numpy as jnp
import numpy as np
from jax import lax
from jax.experimental import pallas as pl
from jax.experimental.pallas import tpu as pltpu
from jax.sharding import Mesh, PartitionSpec as P


D = 2048
NOPE = 128
ROPE = 64
VDIM = 128
QK = 192
SEQS = 4
LANE = 256
BANDS = D // LANE

epsilon = 1e-06
rotary_base = 10000.0
score_scale = QK ** (-0.5) * 1.4426950408889634

Y = ("half", "quad")
ALL = ("half", "quad", "core", "tp")


def rotate(values, positions):
    halfway = values.shape[-1] // 2
    inverse = rotary_base ** (-jnp.arange(halfway, dtype=jnp.float32) / halfway)
    angles = positions.astype(jnp.float32)[:, None] * inverse[None, :]
    angles = angles.reshape((1, angles.shape[0], halfway))
    cosine_values = jnp.cos(angles)
    sine_values = jnp.sin(angles)
    first_half = values[..., :halfway]
    second_half = values[..., halfway:]
    return jnp.concatenate(
        [
            first_half * cosine_values - second_half * sine_values,
            second_half * cosine_values + first_half * sine_values,
        ],
        axis=-1,
    )


def shift(x, axis, by, size):
    if by == 0:
        return x
    return lax.ppermute(x, axis, [(i, (i + by) % size) for i in range(size)])


def swap(x):
    return lax.ppermute(x, "core", [(0, 1), (1, 0)])


def spread(x, by, size):
    pairs = []
    for i in range(size):
        pairs.append((i, (i + by) % size))
        pairs.append((size + i, size + (i - by) % size))
    return lax.ppermute(x, ("core", "tp"), pairs)


def dot(a, b):
    return lax.dot_general(a, b, (((1,), (0,)), ((), ())), preferred_element_type=jnp.float32)


def packing(inverse):
    i = lax.broadcasted_iota(jnp.int32, (256, 256), 1 if inverse else 0)
    k = lax.broadcasted_iota(jnp.int32, (256, 256), 0 if inverse else 1)
    d, r = i // 16, i % 16
    return (k == (r // 2) * 32 + (r % 2) * 16 + d).astype(jnp.bfloat16)


def pack_rows(rows_ref, out_ref, perm):
    for b in range(8):
        stack = []
        for j in range(BANDS):
            for slot in range(2):
                lo = slot * 128 + b * 16
                stack.append(rows_ref[lo : lo + 16, j * LANE : (j + 1) * LANE])
        out_ref[b * 256 : (b + 1) * 256, :] = dot(perm, jnp.concatenate(stack, axis=0)).astype(
            jnp.bfloat16
        )


def unpack_rows(in_ref, rows_ref, perm):
    for b in range(8):
        block = dot(perm, in_ref[b * 256 : (b + 1) * 256, :]).astype(jnp.bfloat16)
        for j in range(BANDS):
            for slot in range(2):
                lo = slot * 128 + b * 16
                at = j * 32 + slot * 16
                rows_ref[lo : lo + 16, j * LANE : (j + 1) * LANE] = block[at : at + 16, :]


def places(meta):
    rows = meta.shape[0]
    expert = lax.broadcasted_iota(jnp.int32, (rows, 128), 1).astype(jnp.float32)
    first = (meta[:, 0:1] == expert).astype(jnp.float32)
    second = (meta[:, 1:2] == expert).astype(jnp.float32)
    earlier = (
        lax.broadcasted_iota(jnp.int32, (rows, rows), 0)
        > lax.broadcasted_iota(jnp.int32, (rows, rows), 1)
    ).astype(jnp.bfloat16)
    before = dot(earlier, (first + second).astype(jnp.bfloat16))
    return first, second, before


def load_keys(src, keys, values):
    for j in range(8):
        lo, hi = j * 96, 768 + j * 96
        keys[lo : lo + 96, 0:128] = src[j, 0:96, :]
        keys[hi : hi + 96, 0:128] = src[j, 96:192, :]
        values[lo : lo + 96, :] = src[j, 192:288, :]
        values[hi : hi + 96, :] = src[j, 288:384, :]
        rot = src[j, 384:480, :]
        keys[lo : lo + 96, 128:256] = rot
        keys[hi : hi + 96, 128:256] = pltpu.roll(rot.astype(jnp.float32), 64, 1).astype(
            jnp.bfloat16
        )


def load_query(q_ref, n):
    base = n * 288
    rot = q_ref[base + 192 : base + 288, :].astype(jnp.float32)
    low = lax.broadcasted_iota(jnp.int32, rot.shape, 1) < ROPE
    first = jnp.where(low, rot, 0.0).astype(jnp.bfloat16)
    second = jnp.where(low, pltpu.roll(rot, 64, 1), 0.0).astype(jnp.bfloat16)
    rot = jnp.concatenate([first, second], axis=0)
    return jnp.concatenate([q_ref[base : base + 192, :], rot], axis=1)


def attend(q, keys, values):
    scores = lax.dot_general(
        q, keys[...], (((1,), (1,)), ((), ())), preferred_element_type=jnp.float32
    )
    highest = jnp.max(scores, axis=-1, keepdims=True)
    weights = jnp.exp2((scores - highest) * score_scale)
    totals = jnp.sum(weights, axis=-1, keepdims=True)
    return highest, totals, dot(weights.astype(jnp.bfloat16), values[...])


def attention_near_body(q_ref, a_ref, acc_ref, stat_ref, keys, values):
    load_keys(a_ref, keys, values)
    for n in range(4):
        highest, totals, out = attend(load_query(q_ref, n), keys, values)
        acc_ref[n] = out
        stat_ref[n] = jnp.concatenate([highest + jnp.zeros_like(out), totals + jnp.zeros_like(out)], axis=1)


def attention_far_body(at_ref, q_ref, b_ref, acc_ref, stat_ref, o_ref, keys, values):
    quad = at_ref[2]
    load_keys(b_ref, keys, values)
    for n in range(4):
        highest, totals, out = attend(load_query(q_ref, n), keys, values)
        before, sums = stat_ref[n, :, 0:128], stat_ref[n, :, 128:256]
        top = jnp.maximum(highest, before)
        old = jnp.exp2((before - top) * score_scale)
        new = jnp.exp2((highest - top) * score_scale)
        out = (acc_ref[n] * old + out * new) / (sums * old + totals * new)
        o_ref[(quad + 4 - n) % 4] = out.astype(jnp.bfloat16)


def project_body(
    at_ref,
    att_ref,
    w0,
    w1,
    w2,
    w3,
    s1,
    s2,
    s3,
    w4,
    s4,
    res_ref,
    gain_ref,
    meta_ref,
    stream_ref,
    out_ref,
    rows,
):
    tp, core = at_ref[0], at_ref[1]
    turn = 1 - 2 * core
    last = att_ref[(tp + 4) % 8]
    turned = pltpu.roll(last.astype(jnp.float32), 64, 1).astype(jnp.bfloat16)
    last = jnp.where(core == 0, last, turned)
    near = jnp.concatenate([att_ref[tp], last], axis=1)
    projected = dot(near, jnp.concatenate([w0[...], w4[...], s4[...]], axis=0))
    for k, w_ref, s_ref in ((1, w1, s1), (2, w2, s2), (3, w3, s3)):
        pair = jnp.concatenate(
            [att_ref[(tp + 8 - turn * k) % 8], att_ref[(tp + 8 + turn * k) % 8]], axis=1
        )
        projected += dot(pair, jnp.concatenate([w_ref[...], s_ref[...]], axis=0))
    stream = (res_ref[...].astype(jnp.float32) + projected).astype(jnp.bfloat16)
    stream_ref[...] = stream
    wide = stream.astype(jnp.float32)
    normed = (
        wide * lax.rsqrt(jnp.mean(wide * wide, axis=-1, keepdims=True) + epsilon) * gain_ref[...]
    ).astype(jnp.bfloat16)
    first, second, before = places(meta_ref[...])
    both = first + second
    for slot in range(2):
        pick = (both * (before == slot).astype(jnp.float32)).T.astype(jnp.bfloat16)
        rows[slot * 128 : (slot + 1) * 128, :] = dot(pick, normed).astype(jnp.bfloat16)
    pack_rows(rows, out_ref, packing(False))


def expert_body(in_ref, gate_ref, up_ref, down_ref, out_ref, rows, acc):
    step = pl.program_id(0)

    @pl.when(step == 0)
    def _():
        unpack_rows(in_ref, rows, packing(True))

    x = rows[...]
    gate = dot(x, gate_ref[...])
    up = dot(x, up_ref[...])
    hidden = (gate / (1.0 + jnp.exp(-gate)) * up).astype(jnp.bfloat16)
    part = dot(hidden, down_ref[...])

    @pl.when(step == 0)
    def _():
        acc[...] = part

    @pl.when(step > 0)
    def _():
        acc[...] += part

    @pl.when(step == pl.num_programs(0) - 1)
    def _():
        rows[...] = acc[...].astype(jnp.bfloat16)
        pack_rows(rows, out_ref, packing(False))


def combine_body(in_ref, stream_ref, meta_ref, out_ref, rows):
    unpack_rows(in_ref, rows, packing(True))
    meta = meta_ref[...]
    first, second, before = places(meta)
    logits = meta[:, 2:4]
    weights = jnp.exp(logits - jnp.max(logits, axis=-1, keepdims=True))
    mixing = weights / jnp.sum(weights, axis=-1, keepdims=True) * meta[:, 4:5]
    slots = [(before == slot).astype(jnp.float32) for slot in range(2)]
    total = stream_ref[...].astype(jnp.float32)
    r = rows[...]
    added = None
    for k, hot in enumerate((first, second)):
        pick = jnp.concatenate([hot * slots[0], hot * slots[1]], axis=-1).astype(jnp.bfloat16)
        term = dot(pick, r) * mixing[:, k : k + 1]
        added = term if added is None else added + term
    out_ref[...] = (total + added).astype(jnp.bfloat16)


def vmem(*shape):
    return pltpu.VMEM(shape, jnp.bfloat16)


def params():
    return pltpu.CompilerParams(vmem_limit_bytes=56 * 1024 * 1024)


def kernel_call(body, **options):
    return pl.pallas_call(body, compiler_params=params(), **options)


VM = pl.BlockSpec(memory_space=pltpu.VMEM)
SM = pl.BlockSpec(memory_space=pltpu.SMEM)


def layer(
    residual,
    query,
    latent,
    rope_key,
    latent_gain,
    key_up,
    value_up,
    out_weight,
    norm_gain,
    group_prob,
    pair_logits,
    routes,
    w_gate,
    w_up,
    w_down,
):
    tp = lax.axis_index("tp")
    core = lax.axis_index("core")
    block = query.shape[0]
    rows = residual.shape[0] * SEQS
    tp_size = lax.axis_size("tp")
    quad = lax.axis_index("quad")
    at = jnp.stack([tp, core, quad]).astype(jnp.int32)

    spot = (lax.axis_index("half") * 4 + lax.axis_index("quad")) * 2 + core
    positions = spot * block + jnp.arange(block, dtype=jnp.int32)
    q = jnp.swapaxes(query, 0, 1)
    q_rot = rotate(q[..., NOPE:].astype(jnp.float32), positions).astype(jnp.bfloat16)
    q_rot = jnp.concatenate([q_rot[:, : block // 2], q_rot[:, block // 2 :]], axis=-1)
    q = jnp.concatenate([q[..., :NOPE], q_rot], axis=1)
    queries = []
    for k in range(4):
        piece = lax.dynamic_index_in_dim(q, (quad + k) % 4, 0, keepdims=False)
        queries.append(shift(piece, "quad", k, 4))
    queries = jnp.concatenate(queries, axis=0)

    lat = jnp.swapaxes(latent, 0, 1).astype(jnp.float32)
    lat = (
        lat * lax.rsqrt(jnp.mean(lat * lat, axis=-1, keepdims=True) + epsilon) * latent_gain
    ).astype(jnp.bfloat16)
    keys = jnp.einsum("spd,dc->spc", lat, key_up, preferred_element_type=jnp.float32)
    vals = jnp.einsum("spd,dc->spc", lat, value_up, preferred_element_type=jnp.float32)
    rot = rotate(jnp.swapaxes(rope_key, 0, 1).astype(jnp.float32), positions)
    rot = jnp.concatenate([rot[:, : block // 2], rot[:, block // 2 :]], axis=-1)
    kv = jnp.concatenate([keys, vals, rot], axis=1).astype(jnp.bfloat16)
    kv = jnp.concatenate([kv, kv], axis=0)
    half_rows = out_weight.shape[0] // 2
    one, two = spread(out_weight, 1, tp_size), spread(out_weight, 2, tp_size)
    three = spread(two, 1, tp_size)
    part = lax.dynamic_slice(two, (core * half_rows, 0), (half_rows, D))
    four = spread(part, 2, tp_size)
    weights = [out_weight, one, two, three, swap(one), swap(two)]
    weights += [swap(three), four, swap(four)]

    near = lax.all_to_all(kv, Y, split_axis=0, concat_axis=0, tiled=True)
    far = swap(near)

    scratch = [vmem(8 * block, 256), vmem(8 * block, VDIM)]
    partial, stats = kernel_call(
        attention_near_body,
        out_shape=(
            jax.ShapeDtypeStruct((4, block, VDIM), jnp.float32),
            jax.ShapeDtypeStruct((4, block, 2 * VDIM), jnp.float32),
        ),
        in_specs=[VM] * 2,
        out_specs=(VM, VM),
        scratch_shapes=scratch,
    )(queries, near)
    attended = kernel_call(
        attention_far_body,
        out_shape=jax.ShapeDtypeStruct((4, block, VDIM), jnp.bfloat16),
        in_specs=[SM] + [VM] * 4,
        out_specs=VM,
        scratch_shapes=scratch,
    )(at, queries, far, partial, stats)
    attended = attended.reshape(4 * tp_size, block // tp_size, VDIM)
    attended = lax.all_to_all(attended, ("quad", "tp"), split_axis=0, concat_axis=0, tiled=True)
    attended = attended.reshape(SEQS, tp_size, block // tp_size, VDIM)
    attended = jnp.swapaxes(attended, 0, 1).reshape(tp_size, rows, VDIM)

    res = jnp.swapaxes(residual, 0, 1).reshape(rows, D)
    meta = jnp.concatenate(
        [routes.astype(jnp.float32), pair_logits, group_prob[..., None]], axis=-1
    )
    meta = jnp.swapaxes(meta, 0, 1).reshape(rows, 5)
    stream, outgoing = pl.pallas_call(
        project_body,
        out_shape=(
            jax.ShapeDtypeStruct((rows, D), jnp.bfloat16),
            jax.ShapeDtypeStruct((2048, LANE), jnp.bfloat16),
        ),
        in_specs=[SM] + [VM] * 13,
        out_specs=(VM, VM),
        scratch_shapes=[vmem(256, D)],
        compiler_params=params(),
        name="project",
    )(at, attended, *weights, res, norm_gain.reshape(1, D), meta)

    def exchange(x):
        x = x.reshape(128, 16, LANE)
        return lax.all_to_all(x, ALL, split_axis=0, concat_axis=0, tiled=True).reshape(2048, LANE)

    arrived = exchange(outgoing)
    hidden = w_gate.shape[2]
    step = 256
    served = pl.pallas_call(
        expert_body,
        out_shape=jax.ShapeDtypeStruct((2048, LANE), jnp.bfloat16),
        grid=(hidden // step,),
        in_specs=[
            pl.BlockSpec((2048, LANE), lambda i: (0, 0)),
            pl.BlockSpec((D, step), lambda i: (0, i)),
            pl.BlockSpec((D, step), lambda i: (0, i)),
            pl.BlockSpec((step, D), lambda i: (i, 0)),
        ],
        out_specs=pl.BlockSpec((2048, LANE), lambda i: (0, 0)),
        scratch_shapes=[vmem(256, D), pltpu.VMEM((256, D), jnp.float32)],
        compiler_params=params(),
        name="experts",
    )(arrived, w_gate[0], w_up[0], w_down[0])
    returned = exchange(served)
    combined = pl.pallas_call(
        combine_body,
        out_shape=jax.ShapeDtypeStruct((rows, D), jnp.bfloat16),
        in_specs=[VM] * 3,
        out_specs=VM,
        scratch_shapes=[vmem(256, D)],
        compiler_params=params(),
        name="combine",
    )(returned, stream, meta)
    return jnp.swapaxes(combined.reshape(SEQS, rows // SEQS, D), 0, 1)


def solution(mesh):
    shape = mesh.shape
    devices = np.asarray(mesh.devices).reshape(
        shape["grp"], 2, 4, shape["sp"] // 8, shape["tp"]
    )
    fine = Mesh(devices, ("grp", "half", "quad", "core", "tp"))
    sp = ("half", "quad", "core")
    both = ("half", "quad", "core", "tp")
    placed = (
        P(both, "grp", None),
        P(sp, "grp", "tp"),
        P(sp, "grp", None),
        P(sp, "grp", None),
        P(),
        P(None, "tp"),
        P(None, "tp"),
        P("tp", None),
        P(),
        P(both, "grp"),
        P(both, "grp", None),
        P(both, "grp", None),
        P(both, None, None),
        P(both, None, None),
        P(both, None, None),
    )
    return jax.shard_map(
        layer, mesh=fine, in_specs=placed, out_specs=P(both, "grp", None), check_vma=False
    )
```

```python
import jax
import jax.numpy as jnp
import numpy as np
from jax import lax
from jax.experimental import pallas as pl
from jax.experimental.pallas import tpu as pltpu
from jax.sharding import Mesh, PartitionSpec as P


D = 2048
NOPE = 128
ROPE = 64
VDIM = 128
QK = 192
SEQS = 4
LANE = 256
BANDS = D // LANE

epsilon = 1e-06
rotary_base = 10000.0
score_scale = QK ** (-0.5) * 1.4426950408889634

Y = ("half", "quad")
ALL = ("half", "quad", "core", "tp")


def rotate(values, positions):
    halfway = values.shape[-1] // 2
    inverse = rotary_base ** (-jnp.arange(halfway, dtype=jnp.float32) / halfway)
    angles = positions.astype(jnp.float32)[:, None] * inverse[None, :]
    angles = angles.reshape((1, angles.shape[0], halfway))
    cosine_values = jnp.cos(angles)
    sine_values = jnp.sin(angles)
    first_half = values[..., :halfway]
    second_half = values[..., halfway:]
    return jnp.concatenate(
        [
            first_half * cosine_values - second_half * sine_values,
            second_half * cosine_values + first_half * sine_values,
        ],
        axis=-1,
    )


def shift(x, axis, by, size):
    if by == 0:
        return x
    return lax.ppermute(x, axis, [(i, (i + by) % size) for i in range(size)])


def swap(x):
    return lax.ppermute(x, "core", [(0, 1), (1, 0)])


def spread(x, by, size):
    pairs = []
    for i in range(size):
        pairs.append((i, (i + by) % size))
        pairs.append((size + i, size + (i - by) % size))
    return lax.ppermute(x, ("core", "tp"), pairs)


def dot(a, b):
    return lax.dot_general(a, b, (((1,), (0,)), ((), ())), preferred_element_type=jnp.float32)


def packing(inverse):
    i = lax.broadcasted_iota(jnp.int32, (256, 256), 1 if inverse else 0)
    k = lax.broadcasted_iota(jnp.int32, (256, 256), 0 if inverse else 1)
    d, r = i // 16, i % 16
    return (k == (r // 2) * 32 + (r % 2) * 16 + d).astype(jnp.bfloat16)


def pack_rows(rows_ref, out_ref, perm):
    for b in range(8):
        stack = []
        for j in range(BANDS):
            for slot in range(2):
                lo = slot * 128 + b * 16
                stack.append(rows_ref[lo : lo + 16, j * LANE : (j + 1) * LANE])
        out_ref[b * 256 : (b + 1) * 256, :] = dot(perm, jnp.concatenate(stack, axis=0)).astype(
            jnp.bfloat16
        )


def unpack_rows(in_ref, rows_ref, perm):
    for b in range(8):
        block = dot(perm, in_ref[b * 256 : (b + 1) * 256, :]).astype(jnp.bfloat16)
        for j in range(BANDS):
            for slot in range(2):
                lo = slot * 128 + b * 16
                at = j * 32 + slot * 16
                rows_ref[lo : lo + 16, j * LANE : (j + 1) * LANE] = block[at : at + 16, :]


def places(meta):
    rows = meta.shape[0]
    expert = lax.broadcasted_iota(jnp.int32, (rows, 128), 1).astype(jnp.float32)
    first = (meta[:, 0:1] == expert).astype(jnp.float32)
    second = (meta[:, 1:2] == expert).astype(jnp.float32)
    earlier = (
        lax.broadcasted_iota(jnp.int32, (rows, rows), 0)
        > lax.broadcasted_iota(jnp.int32, (rows, rows), 1)
    ).astype(jnp.bfloat16)
    before = dot(earlier, (first + second).astype(jnp.bfloat16))
    return first, second, before


def load_keys(src, keys, values):
    for j in range(8):
        lo, hi = j * 96, 768 + j * 96
        keys[lo : lo + 96, 0:128] = src[j, 0:96, :]
        keys[hi : hi + 96, 0:128] = src[j, 96:192, :]
        values[lo : lo + 96, :] = src[j, 192:288, :]
        values[hi : hi + 96, :] = src[j, 288:384, :]
        rot = src[j, 384:480, :]
        keys[lo : lo + 96, 128:256] = rot
        keys[hi : hi + 96, 128:256] = pltpu.roll(rot.astype(jnp.float32), 64, 1).astype(
            jnp.bfloat16
        )


def load_query(q_ref, n):
    base = n * 288
    rot = q_ref[base + 192 : base + 288, :].astype(jnp.float32)
    low = lax.broadcasted_iota(jnp.int32, rot.shape, 1) < ROPE
    first = jnp.where(low, rot, 0.0).astype(jnp.bfloat16)
    second = jnp.where(low, pltpu.roll(rot, 64, 1), 0.0).astype(jnp.bfloat16)
    rot = jnp.concatenate([first, second], axis=0)
    return jnp.concatenate([q_ref[base : base + 192, :], rot], axis=1)


def attend(q, keys, values):
    scores = lax.dot_general(
        q, keys[...], (((1,), (1,)), ((), ())), preferred_element_type=jnp.float32
    )
    highest = jnp.max(scores, axis=-1, keepdims=True)
    weights = jnp.exp2((scores - highest) * score_scale)
    totals = jnp.sum(weights, axis=-1, keepdims=True)
    return highest, totals, dot(weights.astype(jnp.bfloat16), values[...])


def attention_near_body(q_ref, a_ref, acc_ref, stat_ref, keys, values):
    load_keys(a_ref, keys, values)
    for n in range(4):
        highest, totals, out = attend(load_query(q_ref, n), keys, values)
        acc_ref[n] = out
        stat_ref[n] = jnp.concatenate([highest + jnp.zeros_like(out), totals + jnp.zeros_like(out)], axis=1)


def attention_far_body(at_ref, q_ref, b_ref, acc_ref, stat_ref, o_ref, keys, values):
    quad = at_ref[2]
    load_keys(b_ref, keys, values)
    for n in range(4):
        highest, totals, out = attend(load_query(q_ref, n), keys, values)
        before, sums = stat_ref[n, :, 0:128], stat_ref[n, :, 128:256]
        top = jnp.maximum(highest, before)
        old = jnp.exp2((before - top) * score_scale)
        new = jnp.exp2((highest - top) * score_scale)
        out = (acc_ref[n] * old + out * new) / (sums * old + totals * new)
        o_ref[(quad + 4 - n) % 4] = out.astype(jnp.bfloat16)


def project_body(
    at_ref,
    att_ref,
    w0,
    w1,
    w2,
    w3,
    s1,
    s2,
    s3,
    w4,
    s4,
    res_ref,
    gain_ref,
    meta_ref,
    stream_ref,
    out_ref,
    rows,
):
    tp, core = at_ref[0], at_ref[1]
    turn = 1 - 2 * core
    last = att_ref[(tp + 4) % 8]
    turned = pltpu.roll(last.astype(jnp.float32), 64, 1).astype(jnp.bfloat16)
    last = jnp.where(core == 0, last, turned)
    near = jnp.concatenate([att_ref[tp], last], axis=1)
    projected = dot(near, jnp.concatenate([w0[...], w4[...], s4[...]], axis=0))
    for k, w_ref, s_ref in ((1, w1, s1), (2, w2, s2), (3, w3, s3)):
        pair = jnp.concatenate(
            [att_ref[(tp + 8 - turn * k) % 8], att_ref[(tp + 8 + turn * k) % 8]], axis=1
        )
        projected += dot(pair, jnp.concatenate([w_ref[...], s_ref[...]], axis=0))
    stream = (res_ref[...].astype(jnp.float32) + projected).astype(jnp.bfloat16)
    stream_ref[...] = stream
    wide = stream.astype(jnp.float32)
    normed = (
        wide * lax.rsqrt(jnp.mean(wide * wide, axis=-1, keepdims=True) + epsilon) * gain_ref[...]
    ).astype(jnp.bfloat16)
    first, second, before = places(meta_ref[...])
    both = first + second
    for slot in range(2):
        pick = (both * (before == slot).astype(jnp.float32)).T.astype(jnp.bfloat16)
        rows[slot * 128 : (slot + 1) * 128, :] = dot(pick, normed).astype(jnp.bfloat16)
    pack_rows(rows, out_ref, packing(False))


def expert_body(in_ref, gate_ref, up_ref, down_ref, out_ref, rows):
    unpack_rows(in_ref, rows, packing(True))
    x = rows[...]
    hid = []
    for n in range(0, gate_ref.shape[1], 256):
        gate = dot(x, gate_ref[:, n : n + 256])
        up = dot(x, up_ref[:, n : n + 256])
        hidden = (gate / (1.0 + jnp.exp(-gate)) * up).astype(jnp.bfloat16)
        hid.append(hidden)
    hidden = jnp.concatenate(hid, axis=1)
    for n in range(0, D, 512):
        rows[:, n : n + 512] = dot(hidden, down_ref[:, n : n + 512]).astype(jnp.bfloat16)
    pack_rows(rows, out_ref, packing(False))


def combine_body(in_ref, stream_ref, meta_ref, out_ref, rows):
    unpack_rows(in_ref, rows, packing(True))
    meta = meta_ref[...]
    first, second, before = places(meta)
    logits = meta[:, 2:4]
    weights = jnp.exp(logits - jnp.max(logits, axis=-1, keepdims=True))
    mixing = weights / jnp.sum(weights, axis=-1, keepdims=True) * meta[:, 4:5]
    slots = [(before == slot).astype(jnp.float32) for slot in range(2)]
    total = stream_ref[...].astype(jnp.float32)
    r = rows[...]
    added = None
    for k, hot in enumerate((first, second)):
        pick = jnp.concatenate([hot * slots[0], hot * slots[1]], axis=-1).astype(jnp.bfloat16)
        term = dot(pick, r) * mixing[:, k : k + 1]
        added = term if added is None else added + term
    out_ref[...] = (total + added).astype(jnp.bfloat16)


def vmem(*shape):
    return pltpu.VMEM(shape, jnp.bfloat16)


def params(mib):
    return pltpu.CompilerParams(vmem_limit_bytes=mib * 1024 * 1024)


def kernel_call(body, limit, **options):
    return pl.pallas_call(body, compiler_params=params(limit), **options)


VM = pl.BlockSpec(memory_space=pltpu.VMEM)
SM = pl.BlockSpec(memory_space=pltpu.SMEM)


def layer(
    residual,
    query,
    latent,
    rope_key,
    latent_gain,
    key_up,
    value_up,
    out_weight,
    norm_gain,
    group_prob,
    pair_logits,
    routes,
    w_gate,
    w_up,
    w_down,
):
    tp = lax.axis_index("tp")
    core = lax.axis_index("core")
    block = query.shape[0]
    rows = residual.shape[0] * SEQS
    tp_size = lax.axis_size("tp")
    quad = lax.axis_index("quad")
    at = jnp.stack([tp, core, quad]).astype(jnp.int32)

    spot = (lax.axis_index("half") * 4 + lax.axis_index("quad")) * 2 + core
    positions = spot * block + jnp.arange(block, dtype=jnp.int32)
    q = jnp.swapaxes(query, 0, 1)
    q_rot = rotate(q[..., NOPE:].astype(jnp.float32), positions).astype(jnp.bfloat16)
    q_rot = jnp.concatenate([q_rot[:, : block // 2], q_rot[:, block // 2 :]], axis=-1)
    q = jnp.concatenate([q[..., :NOPE], q_rot], axis=1)
    queries = []
    for k in range(4):
        piece = lax.dynamic_index_in_dim(q, (quad + k) % 4, 0, keepdims=False)
        queries.append(shift(piece, "quad", k, 4))
    queries = jnp.concatenate(queries, axis=0)

    lat = jnp.swapaxes(latent, 0, 1).astype(jnp.float32)
    lat = (
        lat * lax.rsqrt(jnp.mean(lat * lat, axis=-1, keepdims=True) + epsilon) * latent_gain
    ).astype(jnp.bfloat16)
    keys = jnp.einsum("spd,dc->spc", lat, key_up, preferred_element_type=jnp.float32)
    vals = jnp.einsum("spd,dc->spc", lat, value_up, preferred_element_type=jnp.float32)
    rot = rotate(jnp.swapaxes(rope_key, 0, 1).astype(jnp.float32), positions)
    rot = jnp.concatenate([rot[:, : block // 2], rot[:, block // 2 :]], axis=-1)
    kv = jnp.concatenate([keys, vals, rot], axis=1).astype(jnp.bfloat16)
    kv = jnp.concatenate([kv, kv], axis=0)
    kv, at = lax.optimization_barrier((kv, at))
    half_rows = out_weight.shape[0] // 2
    one, two = spread(out_weight, 1, tp_size), spread(out_weight, 2, tp_size)
    three = spread(two, 1, tp_size)
    part = lax.dynamic_slice(two, (core * half_rows, 0), (half_rows, D))
    four = spread(part, 2, tp_size)
    weights = [out_weight, one, two, three, swap(one), swap(two)]
    weights += [swap(three), four, swap(four)]

    near = lax.all_to_all(kv, Y, split_axis=0, concat_axis=0, tiled=True)
    far = swap(near)

    scratch = [vmem(8 * block, 256), vmem(8 * block, VDIM)]
    partial, stats = kernel_call(
        attention_near_body,
        limit=12,
        out_shape=(
            jax.ShapeDtypeStruct((4, block, VDIM), jnp.float32),
            jax.ShapeDtypeStruct((4, block, 2 * VDIM), jnp.float32),
        ),
        in_specs=[VM] * 2,
        out_specs=(VM, VM),
        scratch_shapes=scratch,
    )(queries, near)
    attended = kernel_call(
        attention_far_body,
        limit=12,
        out_shape=jax.ShapeDtypeStruct((4, block, VDIM), jnp.bfloat16),
        in_specs=[SM] + [VM] * 4,
        out_specs=VM,
        scratch_shapes=scratch,
    )(at, queries, far, partial, stats)
    attended = attended.reshape(4 * tp_size, block // tp_size, VDIM)
    attended = lax.all_to_all(attended, ("quad", "tp"), split_axis=0, concat_axis=0, tiled=True)
    attended = attended.reshape(SEQS, tp_size, block // tp_size, VDIM)
    attended = jnp.swapaxes(attended, 0, 1).reshape(tp_size, rows, VDIM)

    res = jnp.swapaxes(residual, 0, 1).reshape(rows, D)
    meta = jnp.concatenate(
        [routes.astype(jnp.float32), pair_logits, group_prob[..., None]], axis=-1
    )
    meta = jnp.swapaxes(meta, 0, 1).reshape(rows, 5)
    stream, outgoing = kernel_call(
        project_body,
        limit=10,
        out_shape=(
            jax.ShapeDtypeStruct((rows, D), jnp.bfloat16),
            jax.ShapeDtypeStruct((2048, LANE), jnp.bfloat16),
        ),
        in_specs=[SM] + [VM] * 13,
        out_specs=(VM, VM),
        scratch_shapes=[vmem(256, D)],
    )(at, attended, *weights, res, norm_gain.reshape(1, D), meta)

    def exchange(x):
        x = x.reshape(128, 16, LANE)
        return lax.all_to_all(x, ALL, split_axis=0, concat_axis=0, tiled=True).reshape(2048, LANE)

    arrived = exchange(outgoing)
    served = kernel_call(
        expert_body,
        limit=10,
        out_shape=jax.ShapeDtypeStruct((2048, LANE), jnp.bfloat16),
        in_specs=[VM] * 4,
        out_specs=VM,
        scratch_shapes=[vmem(256, D)],
    )(arrived, w_gate[0], w_up[0], w_down[0])
    returned = exchange(served)
    combined = kernel_call(
        combine_body,
        limit=8,
        out_shape=jax.ShapeDtypeStruct((rows, D), jnp.bfloat16),
        in_specs=[VM] * 3,
        out_specs=VM,
        scratch_shapes=[vmem(256, D)],
    )(returned, stream, meta)
    return jnp.swapaxes(combined.reshape(SEQS, rows // SEQS, D), 0, 1)


def solution(mesh):
    shape = mesh.shape
    devices = np.asarray(mesh.devices).reshape(
        shape["grp"], 2, 4, shape["sp"] // 8, shape["tp"]
    )
    fine = Mesh(devices, ("grp", "half", "quad", "core", "tp"))
    sp = ("half", "quad", "core")
    both = ("half", "quad", "core", "tp")
    placed = (
        P(both, "grp", None),
        P(sp, "grp", "tp"),
        P(sp, "grp", None),
        P(sp, "grp", None),
        P(),
        P(None, "tp"),
        P(None, "tp"),
        P("tp", None),
        P(),
        P(both, "grp"),
        P(both, "grp", None),
        P(both, "grp", None),
        P(both, None, None),
        P(both, None, None),
        P(both, None, None),
    )
    return jax.shard_map(
        layer, mesh=fine, in_specs=placed, out_specs=P(both, "grp", None), check_vma=False
    )
```

```python
import jax
import jax.numpy as jnp
import numpy as np
from jax import lax
from jax.experimental import pallas as pl
from jax.experimental.pallas import tpu as pltpu
from jax.sharding import Mesh, PartitionSpec as P


D = 2048
NOPE = 128
ROPE = 64
VDIM = 128
QK = 192
SEQS = 4
LANE = 256
BANDS = D // LANE

epsilon = 1e-06
rotary_base = 10000.0
score_scale = QK ** (-0.5) * 1.4426950408889634

Y = ("half", "quad")
ALL = ("half", "quad", "core", "tp")


def rotate(values, positions):
    halfway = values.shape[-1] // 2
    inverse = rotary_base ** (-jnp.arange(halfway, dtype=jnp.float32) / halfway)
    angles = positions.astype(jnp.float32)[:, None] * inverse[None, :]
    angles = angles.reshape((1, angles.shape[0], halfway))
    cosine_values = jnp.cos(angles)
    sine_values = jnp.sin(angles)
    first_half = values[..., :halfway]
    second_half = values[..., halfway:]
    return jnp.concatenate(
        [
            first_half * cosine_values - second_half * sine_values,
            second_half * cosine_values + first_half * sine_values,
        ],
        axis=-1,
    )


def shift(x, axis, by, size):
    if by == 0:
        return x
    return lax.ppermute(x, axis, [(i, (i + by) % size) for i in range(size)])


def swap(x):
    return lax.ppermute(x, "core", [(0, 1), (1, 0)])


def spread(x, by, size):
    pairs = []
    for i in range(size):
        pairs.append((i, (i + by) % size))
        pairs.append((size + i, size + (i - by) % size))
    return lax.ppermute(x, ("core", "tp"), pairs)


def dot(a, b):
    return lax.dot_general(a, b, (((1,), (0,)), ((), ())), preferred_element_type=jnp.float32)


def packing(inverse):
    i = lax.broadcasted_iota(jnp.int32, (256, 256), 1 if inverse else 0)
    k = lax.broadcasted_iota(jnp.int32, (256, 256), 0 if inverse else 1)
    d, r = i // 16, i % 16
    return (k == (r // 2) * 32 + (r % 2) * 16 + d).astype(jnp.bfloat16)


def pack_rows(rows_ref, out_ref, perm):
    for b in range(8):
        stack = []
        for j in range(BANDS):
            for slot in range(2):
                lo = slot * 128 + b * 16
                stack.append(rows_ref[lo : lo + 16, j * LANE : (j + 1) * LANE])
        out_ref[b * 256 : (b + 1) * 256, :] = dot(perm, jnp.concatenate(stack, axis=0)).astype(
            jnp.bfloat16
        )


def unpack_rows(in_ref, rows_ref, perm):
    for b in range(8):
        block = dot(perm, in_ref[b * 256 : (b + 1) * 256, :]).astype(jnp.bfloat16)
        for j in range(BANDS):
            for slot in range(2):
                lo = slot * 128 + b * 16
                at = j * 32 + slot * 16
                rows_ref[lo : lo + 16, j * LANE : (j + 1) * LANE] = block[at : at + 16, :]


def places(meta):
    rows = meta.shape[0]
    expert = lax.broadcasted_iota(jnp.int32, (rows, 128), 1).astype(jnp.float32)
    first = (meta[:, 0:1] == expert).astype(jnp.float32)
    second = (meta[:, 1:2] == expert).astype(jnp.float32)
    earlier = (
        lax.broadcasted_iota(jnp.int32, (rows, rows), 0)
        > lax.broadcasted_iota(jnp.int32, (rows, rows), 1)
    ).astype(jnp.bfloat16)
    before = dot(earlier, (first + second).astype(jnp.bfloat16))
    return first, second, before


def load_keys(src, keys, values):
    for j in range(8):
        lo, hi = j * 96, 768 + j * 96
        keys[lo : lo + 96, 0:128] = src[j, 0:96, :]
        keys[hi : hi + 96, 0:128] = src[j, 96:192, :]
        values[lo : lo + 96, :] = src[j, 192:288, :]
        values[hi : hi + 96, :] = src[j, 288:384, :]
        rot = src[j, 384:480, :]
        keys[lo : lo + 96, 128:256] = rot
        keys[hi : hi + 96, 128:256] = pltpu.roll(rot.astype(jnp.float32), 64, 1).astype(
            jnp.bfloat16
        )


def load_query(q_ref, n):
    base = n * 288
    rot = q_ref[base + 192 : base + 288, :].astype(jnp.float32)
    low = lax.broadcasted_iota(jnp.int32, rot.shape, 1) < ROPE
    first = jnp.where(low, rot, 0.0).astype(jnp.bfloat16)
    second = jnp.where(low, pltpu.roll(rot, 64, 1), 0.0).astype(jnp.bfloat16)
    rot = jnp.concatenate([first, second], axis=0)
    return jnp.concatenate([q_ref[base : base + 192, :], rot], axis=1)


def attend(q, keys, values):
    scores = lax.dot_general(
        q, keys[...], (((1,), (1,)), ((), ())), preferred_element_type=jnp.float32
    )
    highest = jnp.max(scores, axis=-1, keepdims=True)
    weights = jnp.exp2((scores - highest) * score_scale)
    totals = jnp.sum(weights, axis=-1, keepdims=True)
    return highest, totals, dot(weights.astype(jnp.bfloat16), values[...])


def attention_near_body(q_ref, a_ref, acc_ref, stat_ref, padded_ref, keys, values):
    load_keys(a_ref, keys, values)
    for n in range(4):
        q = load_query(q_ref, n)
        padded_ref[n] = q
        highest, totals, out = attend(q, keys, values)
        acc_ref[n] = out
        stat_ref[n] = jnp.concatenate([highest + jnp.zeros_like(out), totals + jnp.zeros_like(out)], axis=1)


def attention_far_body(at_ref, q_ref, b_ref, acc_ref, stat_ref, o_ref, keys, values):
    quad = at_ref[2]
    load_keys(b_ref, keys, values)
    for n in range(4):
        highest, totals, out = attend(q_ref[n], keys, values)
        before, sums = stat_ref[n, :, 0:128], stat_ref[n, :, 128:256]
        top = jnp.maximum(highest, before)
        old = jnp.exp2((before - top) * score_scale)
        new = jnp.exp2((highest - top) * score_scale)
        out = (acc_ref[n] * old + out * new) / (sums * old + totals * new)
        o_ref[(quad + 4 - n) % 4] = out.astype(jnp.bfloat16)


def project_body(
    at_ref,
    att_ref,
    w0,
    w1,
    w2,
    w3,
    s1,
    s2,
    s3,
    w4,
    s4,
    res_ref,
    gain_ref,
    meta_ref,
    stream_ref,
    out_ref,
    rows,
):
    tp, core = at_ref[0], at_ref[1]
    turn = 1 - 2 * core

    def head(k):
        spot = (tp + 8 + k) % 8
        parts = [att_ref[8 * seq + spot].astype(jnp.float32) for seq in range(SEQS)]
        return jnp.concatenate(parts, axis=0)

    last = head(4)
    last = jnp.where(core == 0, last, pltpu.roll(last, 64, 1))
    lhs = [head(0), last]
    for k in (1, 2, 3):
        lhs += [head(-turn * k), head(turn * k)]
    lhs = jnp.concatenate(lhs, axis=1).astype(jnp.bfloat16)
    count = lhs.shape[0]
    row = lax.broadcasted_iota(jnp.int32, (count, count), 0)
    col = lax.broadcasted_iota(jnp.int32, (count, count), 1)
    turned = (col == row % SEQS * (count // SEQS) + row // SEQS).astype(jnp.bfloat16)
    lhs = dot(turned, lhs).astype(jnp.bfloat16)
    projected = dot(lhs[:, 0:256], jnp.concatenate([w0[...], w4[...], s4[...]], axis=0))
    for n, w_ref, s_ref in ((1, w1, s1), (2, w2, s2), (3, w3, s3)):
        both = jnp.concatenate([w_ref[...], s_ref[...]], axis=0)
        projected += dot(lhs[:, n * 256 : (n + 1) * 256], both)
    stream = (res_ref[...].astype(jnp.float32) + projected).astype(jnp.bfloat16)
    stream_ref[...] = stream
    wide = stream.astype(jnp.float32)
    normed = (
        wide * lax.rsqrt(jnp.mean(wide * wide, axis=-1, keepdims=True) + epsilon) * gain_ref[...]
    ).astype(jnp.bfloat16)
    first, second, before = places(meta_ref[...])
    both = first + second
    for slot in range(2):
        pick = (both * (before == slot).astype(jnp.float32)).T.astype(jnp.bfloat16)
        rows[slot * 128 : (slot + 1) * 128, :] = dot(pick, normed).astype(jnp.bfloat16)
    pack_rows(rows, out_ref, packing(False))


def expert_body(in_ref, gate_ref, up_ref, down_ref, out_ref, rows):
    unpack_rows(in_ref, rows, packing(True))
    x = rows[...]
    hid = []
    for n in range(0, gate_ref.shape[1], 256):
        gate = dot(x, gate_ref[:, n : n + 256])
        up = dot(x, up_ref[:, n : n + 256])
        hidden = (gate / (1.0 + jnp.exp(-gate)) * up).astype(jnp.bfloat16)
        hid.append(hidden)
    hidden = jnp.concatenate(hid, axis=1)
    for n in range(0, D, 512):
        rows[:, n : n + 512] = dot(hidden, down_ref[:, n : n + 512]).astype(jnp.bfloat16)
    pack_rows(rows, out_ref, packing(False))


def combine_body(in_ref, stream_ref, meta_ref, out_ref, rows):
    unpack_rows(in_ref, rows, packing(True))
    meta = meta_ref[...]
    first, second, before = places(meta)
    logits = meta[:, 2:4]
    weights = jnp.exp(logits - jnp.max(logits, axis=-1, keepdims=True))
    mixing = weights / jnp.sum(weights, axis=-1, keepdims=True) * meta[:, 4:5]
    slots = [(before == slot).astype(jnp.float32) for slot in range(2)]
    total = stream_ref[...].astype(jnp.float32)
    r = rows[...]
    added = None
    for k, hot in enumerate((first, second)):
        pick = jnp.concatenate([hot * slots[0], hot * slots[1]], axis=-1).astype(jnp.bfloat16)
        term = dot(pick, r) * mixing[:, k : k + 1]
        added = term if added is None else added + term
    total = (total + added).astype(jnp.bfloat16)
    for p in range(out_ref.shape[0]):
        out_ref[p] = total[SEQS * p : SEQS * (p + 1), :]


def vmem(*shape):
    return pltpu.VMEM(shape, jnp.bfloat16)


def params(mib):
    return pltpu.CompilerParams(vmem_limit_bytes=mib * 1024 * 1024)


def kernel_call(body, limit, **options):
    return pl.pallas_call(body, compiler_params=params(limit), **options)


VM = pl.BlockSpec(memory_space=pltpu.VMEM)
SM = pl.BlockSpec(memory_space=pltpu.SMEM)


def layer(
    residual,
    query,
    latent,
    rope_key,
    latent_gain,
    key_up,
    value_up,
    out_weight,
    norm_gain,
    group_prob,
    pair_logits,
    routes,
    w_gate,
    w_up,
    w_down,
):
    tp = lax.axis_index("tp")
    core = lax.axis_index("core")
    block = query.shape[0]
    rows = residual.shape[0] * SEQS
    tp_size = lax.axis_size("tp")
    quad = lax.axis_index("quad")
    at = jnp.stack([tp, core, quad]).astype(jnp.int32)

    spot = (lax.axis_index("half") * 4 + lax.axis_index("quad")) * 2 + core
    positions = spot * block + jnp.arange(block, dtype=jnp.int32)
    q = jnp.swapaxes(query, 0, 1)
    q_rot = rotate(q[..., NOPE:].astype(jnp.float32), positions).astype(jnp.bfloat16)
    q_rot = jnp.concatenate([q_rot[:, : block // 2], q_rot[:, block // 2 :]], axis=-1)
    q = jnp.concatenate([q[..., :NOPE], q_rot], axis=1)
    res = residual.reshape(rows, D)
    meta = jnp.concatenate(
        [routes.astype(jnp.float32), pair_logits, group_prob[..., None]], axis=-1
    )
    meta = meta.reshape(rows, 5)
    q, res, meta = lax.optimization_barrier((q, res, meta))
    queries = []
    for k in range(4):
        piece = lax.dynamic_index_in_dim(q, (quad + k) % 4, 0, keepdims=False)
        queries.append(shift(piece, "quad", k, 4))
    queries = jnp.concatenate(queries, axis=0)

    lat = jnp.swapaxes(latent, 0, 1).astype(jnp.float32)
    lat = (
        lat * lax.rsqrt(jnp.mean(lat * lat, axis=-1, keepdims=True) + epsilon) * latent_gain
    ).astype(jnp.bfloat16)
    keys = jnp.einsum("spd,dc->spc", lat, key_up, preferred_element_type=jnp.float32)
    vals = jnp.einsum("spd,dc->spc", lat, value_up, preferred_element_type=jnp.float32)
    rot = rotate(jnp.swapaxes(rope_key, 0, 1).astype(jnp.float32), positions)
    rot = jnp.concatenate([rot[:, : block // 2], rot[:, block // 2 :]], axis=-1)
    kv = jnp.concatenate([keys, vals, rot], axis=1).astype(jnp.bfloat16)
    kv = jnp.concatenate([kv, kv], axis=0)
    kv, at = lax.optimization_barrier((kv, at))
    half_rows = out_weight.shape[0] // 2
    one, two = spread(out_weight, 1, tp_size), spread(out_weight, 2, tp_size)
    three = spread(two, 1, tp_size)
    part = lax.dynamic_slice(two, (core * half_rows, 0), (half_rows, D))
    four = spread(part, 2, tp_size)
    weights = [out_weight, one, two, three, swap(one), swap(two)]
    weights += [swap(three), four, swap(four)]

    near = lax.all_to_all(kv, Y, split_axis=0, concat_axis=0, tiled=True)
    far = swap(near)

    scratch = [vmem(8 * block, 256), vmem(8 * block, VDIM)]
    partial, stats, padded = kernel_call(
        attention_near_body,
        limit=12,
        out_shape=(
            jax.ShapeDtypeStruct((4, block, VDIM), jnp.float32),
            jax.ShapeDtypeStruct((4, block, 2 * VDIM), jnp.float32),
            jax.ShapeDtypeStruct((4, block, 256), jnp.bfloat16),
        ),
        in_specs=[VM] * 2,
        out_specs=(VM, VM, VM),
        scratch_shapes=scratch,
    )(queries, near)
    attended = kernel_call(
        attention_far_body,
        limit=12,
        out_shape=jax.ShapeDtypeStruct((4, block, VDIM), jnp.bfloat16),
        in_specs=[SM] + [VM] * 4,
        out_specs=VM,
        scratch_shapes=scratch,
    )(at, padded, far, partial, stats)
    attended = attended.reshape(4 * tp_size, block // tp_size, VDIM)
    attended = lax.all_to_all(attended, ("quad", "tp"), split_axis=0, concat_axis=0, tiled=True)

    stream, outgoing = kernel_call(
        project_body,
        limit=10,
        out_shape=(
            jax.ShapeDtypeStruct((rows, D), jnp.bfloat16),
            jax.ShapeDtypeStruct((2048, LANE), jnp.bfloat16),
        ),
        in_specs=[SM] + [VM] * 13,
        out_specs=(VM, VM),
        scratch_shapes=[vmem(256, D)],
    )(at, attended, *weights, res, norm_gain.reshape(1, D), meta)

    def exchange(x):
        x = x.reshape(128, 16, LANE)
        return lax.all_to_all(x, ALL, split_axis=0, concat_axis=0, tiled=True).reshape(2048, LANE)

    arrived = exchange(outgoing)
    served = kernel_call(
        expert_body,
        limit=10,
        out_shape=jax.ShapeDtypeStruct((2048, LANE), jnp.bfloat16),
        in_specs=[VM] * 4,
        out_specs=VM,
        scratch_shapes=[vmem(256, D)],
    )(arrived, w_gate[0], w_up[0], w_down[0])
    returned = exchange(served)
    combined = kernel_call(
        combine_body,
        limit=8,
        out_shape=jax.ShapeDtypeStruct(residual.shape, jnp.bfloat16),
        in_specs=[VM] * 3,
        out_specs=VM,
        scratch_shapes=[vmem(256, D)],
    )(returned, stream, meta)
    return combined


def solution(mesh):
    shape = mesh.shape
    devices = np.asarray(mesh.devices).reshape(
        shape["grp"], 2, 4, shape["sp"] // 8, shape["tp"]
    )
    fine = Mesh(devices, ("grp", "half", "quad", "core", "tp"))
    sp = ("half", "quad", "core")
    both = ("half", "quad", "core", "tp")
    placed = (
        P(both, "grp", None),
        P(sp, "grp", "tp"),
        P(sp, "grp", None),
        P(sp, "grp", None),
        P(),
        P(None, "tp"),
        P(None, "tp"),
        P("tp", None),
        P(),
        P(both, "grp"),
        P(both, "grp", None),
        P(both, "grp", None),
        P(both, None, None),
        P(both, None, None),
        P(both, None, None),
    )
    return jax.shard_map(
        layer, mesh=fine, in_specs=placed, out_specs=P(both, "grp", None), check_vma=False
    )
```

```python
import jax
import jax.numpy as jnp
import numpy as np
from jax import lax
from jax.experimental import pallas as pl
from jax.experimental.pallas import tpu as pltpu
from jax.sharding import Mesh, PartitionSpec as P


D = 2048
NOPE = 128
ROPE = 64
VDIM = 128
QK = 192
SEQS = 4
LANE = 256
BANDS = D // LANE

epsilon = 1e-06
rotary_base = 10000.0
score_scale = QK ** (-0.5) * 1.4426950408889634

Y = ("half", "quad")
ALL = ("half", "quad", "core", "tp")


def rotate(values, positions):
    halfway = values.shape[-1] // 2
    inverse = rotary_base ** (-jnp.arange(halfway, dtype=jnp.float32) / halfway)
    angles = positions.astype(jnp.float32)[:, None] * inverse[None, :]
    angles = angles.reshape((1, angles.shape[0], halfway))
    cosine_values = jnp.cos(angles)
    sine_values = jnp.sin(angles)
    first_half = values[..., :halfway]
    second_half = values[..., halfway:]
    return jnp.concatenate(
        [
            first_half * cosine_values - second_half * sine_values,
            second_half * cosine_values + first_half * sine_values,
        ],
        axis=-1,
    )


def shift(x, axis, by, size):
    if by == 0:
        return x
    return lax.ppermute(x, axis, [(i, (i + by) % size) for i in range(size)])


def swap(x):
    return lax.ppermute(x, "core", [(0, 1), (1, 0)])


def spread(x, by, size):
    pairs = []
    for i in range(size):
        pairs.append((i, (i + by) % size))
        pairs.append((size + i, size + (i - by) % size))
    return lax.ppermute(x, ("core", "tp"), pairs)


def dot(a, b):
    return lax.dot_general(a, b, (((1,), (0,)), ((), ())), preferred_element_type=jnp.float32)


def packing(inverse):
    i = lax.broadcasted_iota(jnp.int32, (256, 256), 1 if inverse else 0)
    k = lax.broadcasted_iota(jnp.int32, (256, 256), 0 if inverse else 1)
    d, r = i // 16, i % 16
    return (k == (r // 2) * 32 + (r % 2) * 16 + d).astype(jnp.bfloat16)


def pack_rows(rows_ref, out_ref, perm):
    for b in range(8):
        stack = []
        for j in range(BANDS):
            for slot in range(2):
                lo = slot * 128 + b * 16
                stack.append(rows_ref[lo : lo + 16, j * LANE : (j + 1) * LANE])
        out_ref[b * 256 : (b + 1) * 256, :] = dot(perm, jnp.concatenate(stack, axis=0)).astype(
            jnp.bfloat16
        )


def unpack_rows(in_ref, rows_ref, perm):
    for b in range(8):
        block = dot(perm, in_ref[b * 256 : (b + 1) * 256, :]).astype(jnp.bfloat16)
        for j in range(BANDS):
            for slot in range(2):
                lo = slot * 128 + b * 16
                at = j * 32 + slot * 16
                rows_ref[lo : lo + 16, j * LANE : (j + 1) * LANE] = block[at : at + 16, :]


def places(meta):
    rows = meta.shape[0]
    expert = lax.broadcasted_iota(jnp.int32, (rows, 128), 1).astype(jnp.float32)
    first = (meta[:, 0:1] == expert).astype(jnp.float32)
    second = (meta[:, 1:2] == expert).astype(jnp.float32)
    earlier = (
        lax.broadcasted_iota(jnp.int32, (rows, rows), 0)
        > lax.broadcasted_iota(jnp.int32, (rows, rows), 1)
    ).astype(jnp.bfloat16)
    before = dot(earlier, (first + second).astype(jnp.bfloat16))
    return first, second, before


def load_keys(src, keys, values):
    for j in range(8):
        lo, hi = j * 96, 768 + j * 96
        keys[lo : lo + 96, 0:128] = src[j, 0:96, :]
        keys[hi : hi + 96, 0:128] = src[j, 96:192, :]
        values[lo : lo + 96, :] = src[j, 192:288, :]
        values[hi : hi + 96, :] = src[j, 288:384, :]
        rot = src[j, 384:480, :]
        keys[lo : lo + 96, 128:256] = rot
        keys[hi : hi + 96, 128:256] = pltpu.roll(rot.astype(jnp.float32), 64, 1).astype(
            jnp.bfloat16
        )


def load_query(q_ref, n):
    base = n * 288
    rot = q_ref[base + 192 : base + 288, :].astype(jnp.float32)
    low = lax.broadcasted_iota(jnp.int32, rot.shape, 1) < ROPE
    first = jnp.where(low, rot, 0.0).astype(jnp.bfloat16)
    second = jnp.where(low, pltpu.roll(rot, 64, 1), 0.0).astype(jnp.bfloat16)
    rot = jnp.concatenate([first, second], axis=0)
    return jnp.concatenate([q_ref[base : base + 192, :], rot], axis=1)


def attend(q, keys, values):
    scores = lax.dot_general(
        q, keys[...], (((1,), (1,)), ((), ())), preferred_element_type=jnp.float32
    )
    highest = jnp.max(scores, axis=-1, keepdims=True)
    weights = jnp.exp2((scores - highest) * score_scale)
    totals = jnp.sum(weights, axis=-1, keepdims=True)
    return highest, totals, dot(weights.astype(jnp.bfloat16), values[...])


def attention_near_body(q_ref, a_ref, acc_ref, stat_ref, padded_ref, keys, values):
    load_keys(a_ref, keys, values)
    for n in range(4):
        q = load_query(q_ref, n)
        padded_ref[n] = q
        highest, totals, out = attend(q, keys, values)
        acc_ref[n] = out
        stat_ref[n] = jnp.concatenate([highest + jnp.zeros_like(out), totals + jnp.zeros_like(out)], axis=1)


def attention_far_body(at_ref, q_ref, b_ref, acc_ref, stat_ref, o_ref, keys, values):
    quad = at_ref[2]
    load_keys(b_ref, keys, values)
    for n in range(4):
        highest, totals, out = attend(q_ref[n], keys, values)
        before, sums = stat_ref[n, :, 0:128], stat_ref[n, :, 128:256]
        top = jnp.maximum(highest, before)
        old = jnp.exp2((before - top) * score_scale)
        new = jnp.exp2((highest - top) * score_scale)
        out = (acc_ref[n] * old + out * new) / (sums * old + totals * new)
        o_ref[(quad + 4 - n) % 4] = out.astype(jnp.bfloat16)


def project_body(
    at_ref,
    att_ref,
    w0_far,
    w1,
    w2,
    w3,
    s1,
    s2,
    s3,
    w4,
    s4_far,
    res_far,
    gain_ref,
    meta_ref,
    stream_ref,
    out_ref,
    rows,
    w0,
    s4,
    res_ref,
    sems,
):
    pairs = ((w0_far, w0), (s4_far, s4), (res_far, res_ref))
    fetches = [pltpu.make_async_copy(a, b, sems.at[n]) for n, (a, b) in enumerate(pairs)]
    for fetch in fetches:
        fetch.start()
    tp, core = at_ref[0], at_ref[1]
    turn = 1 - 2 * core

    def head(k):
        spot = (tp + 8 + k) % 8
        parts = [att_ref[8 * seq + spot].astype(jnp.float32) for seq in range(SEQS)]
        return jnp.concatenate(parts, axis=0)

    last = head(4)
    last = jnp.where(core == 0, last, pltpu.roll(last, 64, 1))
    lhs = [head(0), last]
    for k in (1, 2, 3):
        lhs += [head(-turn * k), head(turn * k)]
    lhs = jnp.concatenate(lhs, axis=1).astype(jnp.bfloat16)
    count = lhs.shape[0]
    row = lax.broadcasted_iota(jnp.int32, (count, count), 0)
    col = lax.broadcasted_iota(jnp.int32, (count, count), 1)
    turned = (col == row % SEQS * (count // SEQS) + row // SEQS).astype(jnp.bfloat16)
    lhs = dot(turned, lhs).astype(jnp.bfloat16)
    projected = None
    for n, w_ref, s_ref in ((1, w1, s1), (2, w2, s2), (3, w3, s3)):
        both = jnp.concatenate([w_ref[...], s_ref[...]], axis=0)
        part = dot(lhs[:, n * 256 : (n + 1) * 256], both)
        projected = part if projected is None else projected + part
    for fetch in fetches:
        fetch.wait()
    projected += dot(lhs[:, 0:256], jnp.concatenate([w0[...], w4[...], s4[...]], axis=0))
    stream = (res_ref[...].astype(jnp.float32) + projected).astype(jnp.bfloat16)
    stream_ref[...] = stream
    wide = stream.astype(jnp.float32)
    normed = (
        wide * lax.rsqrt(jnp.mean(wide * wide, axis=-1, keepdims=True) + epsilon) * gain_ref[...]
    ).astype(jnp.bfloat16)
    first, second, before = places(meta_ref[...])
    both = first + second
    for slot in range(2):
        pick = (both * (before == slot).astype(jnp.float32)).T.astype(jnp.bfloat16)
        rows[slot * 128 : (slot + 1) * 128, :] = dot(pick, normed).astype(jnp.bfloat16)
    pack_rows(rows, out_ref, packing(False))


def expert_body(in_ref, gate_ref, up_ref, down_ref, out_ref, rows):
    unpack_rows(in_ref, rows, packing(True))
    x = rows[...]
    hid = []
    for n in range(0, gate_ref.shape[1], 256):
        gate = dot(x, gate_ref[:, n : n + 256])
        up = dot(x, up_ref[:, n : n + 256])
        hidden = (gate / (1.0 + jnp.exp(-gate)) * up).astype(jnp.bfloat16)
        hid.append(hidden)
    hidden = jnp.concatenate(hid, axis=1)
    for n in range(0, D, 512):
        rows[:, n : n + 512] = dot(hidden, down_ref[:, n : n + 512]).astype(jnp.bfloat16)
    pack_rows(rows, out_ref, packing(False))


def combine_body(in_ref, stream_ref, meta_ref, out_ref, rows):
    unpack_rows(in_ref, rows, packing(True))
    meta = meta_ref[...]
    first, second, before = places(meta)
    logits = meta[:, 2:4]
    weights = jnp.exp(logits - jnp.max(logits, axis=-1, keepdims=True))
    mixing = weights / jnp.sum(weights, axis=-1, keepdims=True) * meta[:, 4:5]
    slots = [(before == slot).astype(jnp.float32) for slot in range(2)]
    total = stream_ref[...].astype(jnp.float32)
    r = rows[...]
    added = None
    for k, hot in enumerate((first, second)):
        pick = jnp.concatenate([hot * slots[0], hot * slots[1]], axis=-1).astype(jnp.bfloat16)
        term = dot(pick, r) * mixing[:, k : k + 1]
        added = term if added is None else added + term
    total = (total + added).astype(jnp.bfloat16)
    for p in range(out_ref.shape[0]):
        out_ref[p] = total[SEQS * p : SEQS * (p + 1), :]


def meta_body(route_ref, logit_ref, prob_ref, out_ref):
    rows = out_ref.shape[0]
    count = rows // SEQS
    row = lax.broadcasted_iota(jnp.int32, (rows, count), 0)
    col = lax.broadcasted_iota(jnp.int32, (rows, count), 1)
    total = None
    for seq in range(SEQS):
        block = jnp.concatenate(
            [
                route_ref[seq].astype(jnp.float32),
                logit_ref[seq],
                prob_ref[seq : seq + 1, :],
                jnp.zeros((3, count), jnp.float32),
            ],
            axis=0,
        )
        part = lax.dot_general(
            (row == col * SEQS + seq).astype(jnp.float32),
            block,
            (((1,), (1,)), ((), ())),
            precision=lax.Precision.HIGHEST,
            preferred_element_type=jnp.float32,
        )
        total = part if total is None else total + part
    out_ref[...] = total


def vmem(*shape):
    return pltpu.VMEM(shape, jnp.bfloat16)


def params(mib):
    return pltpu.CompilerParams(vmem_limit_bytes=mib * 1024 * 1024)


def kernel_call(body, limit, **options):
    return pl.pallas_call(body, compiler_params=params(limit), **options)


VM = pl.BlockSpec(memory_space=pltpu.VMEM)
SM = pl.BlockSpec(memory_space=pltpu.SMEM)
HB = pl.BlockSpec(memory_space=pltpu.HBM)


def layer(
    residual,
    query,
    latent,
    rope_key,
    latent_gain,
    key_up,
    value_up,
    out_weight,
    norm_gain,
    group_prob,
    pair_logits,
    routes,
    w_gate,
    w_up,
    w_down,
):
    tp = lax.axis_index("tp")
    core = lax.axis_index("core")
    block = query.shape[0]
    rows = residual.shape[0] * SEQS
    tp_size = lax.axis_size("tp")
    quad = lax.axis_index("quad")
    at = jnp.stack([tp, core, quad]).astype(jnp.int32)

    spot = (lax.axis_index("half") * 4 + lax.axis_index("quad")) * 2 + core
    positions = spot * block + jnp.arange(block, dtype=jnp.int32)
    q = jnp.swapaxes(query, 0, 1)
    q_rot = rotate(q[..., NOPE:].astype(jnp.float32), positions).astype(jnp.bfloat16)
    q_rot = jnp.concatenate([q_rot[:, : block // 2], q_rot[:, block // 2 :]], axis=-1)
    q = jnp.concatenate([q[..., :NOPE], q_rot], axis=1)
    res = residual.reshape(rows, D)
    meta = kernel_call(
        meta_body,
        limit=2,
        out_shape=jax.ShapeDtypeStruct((rows, 8), jnp.float32),
        in_specs=[VM] * 3,
        out_specs=VM,
    )(jnp.transpose(routes, (1, 2, 0)), jnp.transpose(pair_logits, (1, 2, 0)), group_prob.T)
    q, res = lax.optimization_barrier((q, res))
    queries = []
    for k in range(4):
        piece = lax.dynamic_index_in_dim(q, (quad + k) % 4, 0, keepdims=False)
        queries.append(shift(piece, "quad", k, 4))
    queries = jnp.concatenate(queries, axis=0)

    lat = jnp.swapaxes(latent, 0, 1).astype(jnp.float32)
    lat = (
        lat * lax.rsqrt(jnp.mean(lat * lat, axis=-1, keepdims=True) + epsilon) * latent_gain
    ).astype(jnp.bfloat16)
    keys = jnp.einsum("spd,dc->spc", lat, key_up, preferred_element_type=jnp.float32)
    vals = jnp.einsum("spd,dc->spc", lat, value_up, preferred_element_type=jnp.float32)
    rot = rotate(jnp.swapaxes(rope_key, 0, 1).astype(jnp.float32), positions)
    rot = jnp.concatenate([rot[:, : block // 2], rot[:, block // 2 :]], axis=-1)
    kv = jnp.concatenate([keys, vals, rot], axis=1).astype(jnp.bfloat16)
    kv = jnp.concatenate([kv, kv], axis=0)
    kv, at = lax.optimization_barrier((kv, at))
    half_rows = out_weight.shape[0] // 2
    one, two = spread(out_weight, 1, tp_size), spread(out_weight, 2, tp_size)
    three = spread(two, 1, tp_size)
    part = lax.dynamic_slice(two, (core * half_rows, 0), (half_rows, D))
    four = spread(part, 2, tp_size)
    weights = [out_weight, one, two, three, swap(one), swap(two)]
    weights += [swap(three), four, swap(four)]

    near = lax.all_to_all(kv, Y, split_axis=0, concat_axis=0, tiled=True)
    far = swap(near)

    scratch = [vmem(8 * block, 256), vmem(8 * block, VDIM)]
    partial, stats, padded = kernel_call(
        attention_near_body,
        limit=12,
        out_shape=(
            jax.ShapeDtypeStruct((4, block, VDIM), jnp.float32),
            jax.ShapeDtypeStruct((4, block, 2 * VDIM), jnp.float32),
            jax.ShapeDtypeStruct((4, block, 256), jnp.bfloat16),
        ),
        in_specs=[VM] * 2,
        out_specs=(VM, VM, VM),
        scratch_shapes=scratch,
    )(queries, near)
    attended = kernel_call(
        attention_far_body,
        limit=12,
        out_shape=jax.ShapeDtypeStruct((4, block, VDIM), jnp.bfloat16),
        in_specs=[SM] + [VM] * 4,
        out_specs=VM,
        scratch_shapes=scratch,
    )(at, padded, far, partial, stats)
    attended = attended.reshape(4 * tp_size, block // tp_size, VDIM)
    attended = lax.all_to_all(attended, ("quad", "tp"), split_axis=0, concat_axis=0, tiled=True)

    stream, outgoing = kernel_call(
        project_body,
        limit=10,
        out_shape=(
            jax.ShapeDtypeStruct((rows, D), jnp.bfloat16),
            jax.ShapeDtypeStruct((2048, LANE), jnp.bfloat16),
        ),
        in_specs=[SM, VM, HB] + [VM] * 7 + [HB, HB, VM, VM],
        out_specs=(VM, VM),
        scratch_shapes=[
            vmem(256, D),
            vmem(*out_weight.shape),
            vmem(half_rows, D),
            vmem(rows, D),
            pltpu.SemaphoreType.DMA((3,)),
        ],
    )(at, attended, *weights, res, norm_gain.reshape(1, D), meta)

    def exchange(x):
        x = x.reshape(128, 16, LANE)
        return lax.all_to_all(x, ALL, split_axis=0, concat_axis=0, tiled=True).reshape(2048, LANE)

    arrived = exchange(outgoing)
    served = kernel_call(
        expert_body,
        limit=10,
        out_shape=jax.ShapeDtypeStruct((2048, LANE), jnp.bfloat16),
        in_specs=[VM] * 4,
        out_specs=VM,
        scratch_shapes=[vmem(256, D)],
    )(arrived, w_gate[0], w_up[0], w_down[0])
    returned = exchange(served)
    combined = kernel_call(
        combine_body,
        limit=8,
        out_shape=jax.ShapeDtypeStruct(residual.shape, jnp.bfloat16),
        in_specs=[VM] * 3,
        out_specs=VM,
        scratch_shapes=[vmem(256, D)],
    )(returned, stream, meta)
    return combined


def solution(mesh):
    shape = mesh.shape
    devices = np.asarray(mesh.devices).reshape(
        shape["grp"], 2, 4, shape["sp"] // 8, shape["tp"]
    )
    fine = Mesh(devices, ("grp", "half", "quad", "core", "tp"))
    sp = ("half", "quad", "core")
    both = ("half", "quad", "core", "tp")
    placed = (
        P(both, "grp", None),
        P(sp, "grp", "tp"),
        P(sp, "grp", None),
        P(sp, "grp", None),
        P(),
        P(None, "tp"),
        P(None, "tp"),
        P("tp", None),
        P(),
        P(both, "grp"),
        P(both, "grp", None),
        P(both, "grp", None),
        P(both, None, None),
        P(both, None, None),
        P(both, None, None),
    )
    return jax.shard_map(
        layer, mesh=fine, in_specs=placed, out_specs=P(both, "grp", None), check_vma=False
    )
```

```python
import jax
import jax.numpy as jnp
import numpy as np
from jax import lax
from jax.experimental import pallas as pl
from jax.experimental.pallas import tpu as pltpu
from jax.sharding import Mesh, PartitionSpec as P


D = 2048
NOPE = 128
ROPE = 64
VDIM = 128
QK = 192
SEQS = 4
LANE = 256
BANDS = D // LANE

epsilon = 1e-06
rotary_base = 10000.0
score_scale = QK ** (-0.5) * 1.4426950408889634

Y = ("half", "quad")
PLANE = ("half", "quad", "tp")


def rotate(values, positions):
    halfway = values.shape[-1] // 2
    inverse = rotary_base ** (-jnp.arange(halfway, dtype=jnp.float32) / halfway)
    angles = positions.astype(jnp.float32)[:, None] * inverse[None, :]
    angles = angles.reshape((1, angles.shape[0], halfway))
    cosine_values = jnp.cos(angles)
    sine_values = jnp.sin(angles)
    first_half = values[..., :halfway]
    second_half = values[..., halfway:]
    return jnp.concatenate(
        [
            first_half * cosine_values - second_half * sine_values,
            second_half * cosine_values + first_half * sine_values,
        ],
        axis=-1,
    )


def shift(x, axis, by, size):
    if by == 0:
        return x
    return lax.ppermute(x, axis, [(i, (i + by) % size) for i in range(size)])


def swap(x):
    return lax.ppermute(x, "core", [(0, 1), (1, 0)])


def spread(x, by, size):
    pairs = []
    for i in range(size):
        pairs.append((i, (i + by) % size))
        pairs.append((size + i, size + (i - by) % size))
    return lax.ppermute(x, ("core", "tp"), pairs)


def dot(a, b):
    return lax.dot_general(a, b, (((1,), (0,)), ((), ())), preferred_element_type=jnp.float32)


def packing(inverse):
    i = lax.broadcasted_iota(jnp.int32, (256, 256), 1 if inverse else 0)
    k = lax.broadcasted_iota(jnp.int32, (256, 256), 0 if inverse else 1)
    d, r = i // 16, i % 16
    return (k == (r // 2) * 32 + (r % 2) * 16 + d).astype(jnp.bfloat16)


def pack_block(rows_ref, b, perm):
    stack = []
    for j in range(BANDS):
        for slot in range(2):
            lo = slot * 128 + b * 16
            stack.append(rows_ref[lo : lo + 16, j * LANE : (j + 1) * LANE])
    return dot(perm, jnp.concatenate(stack, axis=0)).astype(jnp.bfloat16)


def half_of(core):
    return pl.ds(pl.multiple_of(core * 16, 16), 16)


def unpack_rows(own_ref, got_ref, core, rows_ref, perm):
    for b in range(8):
        if b < 4:
            block = own_ref[b * 16 : (b + 1) * 16, half_of(core), :]
        else:
            block = got_ref[(b - 4) * 16 : (b - 3) * 16, :, :]
        block = dot(perm, block.reshape(256, LANE)).astype(jnp.bfloat16)
        for j in range(BANDS):
            for slot in range(2):
                lo = slot * 128 + b * 16
                at = j * 32 + slot * 16
                rows_ref[lo : lo + 16, j * LANE : (j + 1) * LANE] = block[at : at + 16, :]


def pick_body(at_ref, in_ref, out_ref):
    out_ref[...] = in_ref[:, half_of(1 - at_ref[1]), :]


def places(meta):
    rows = meta.shape[0]
    expert = lax.broadcasted_iota(jnp.int32, (rows, 128), 1).astype(jnp.float32)
    first = (meta[:, 0:1] == expert).astype(jnp.float32)
    second = (meta[:, 1:2] == expert).astype(jnp.float32)
    earlier = (
        lax.broadcasted_iota(jnp.int32, (rows, rows), 0)
        > lax.broadcasted_iota(jnp.int32, (rows, rows), 1)
    ).astype(jnp.bfloat16)
    before = dot(earlier, (first + second).astype(jnp.bfloat16))
    return first, second, before


def load_keys(src, keys, values):
    for j in range(8):
        lo, hi = j * 96, 768 + j * 96
        keys[lo : lo + 96, 0:128] = src[j, 0:96, :]
        keys[hi : hi + 96, 0:128] = src[j, 96:192, :]
        values[lo : lo + 96, :] = src[j, 192:288, :]
        values[hi : hi + 96, :] = src[j, 288:384, :]
        rot = src[j, 384:480, :]
        keys[lo : lo + 96, 128:256] = rot
        keys[hi : hi + 96, 128:256] = pltpu.roll(rot.astype(jnp.float32), 64, 1).astype(
            jnp.bfloat16
        )


def load_query(q_ref, n):
    base = n * 288
    rot = q_ref[base + 192 : base + 288, :].astype(jnp.float32)
    low = lax.broadcasted_iota(jnp.int32, rot.shape, 1) < ROPE
    first = jnp.where(low, rot, 0.0).astype(jnp.bfloat16)
    second = jnp.where(low, pltpu.roll(rot, 64, 1), 0.0).astype(jnp.bfloat16)
    rot = jnp.concatenate([first, second], axis=0)
    return jnp.concatenate([q_ref[base : base + 192, :], rot], axis=1)


def attend(q, keys, values):
    scores = lax.dot_general(
        q, keys[...], (((1,), (1,)), ((), ())), preferred_element_type=jnp.float32
    )
    highest = jnp.max(scores, axis=-1, keepdims=True)
    weights = jnp.exp2((scores - highest) * score_scale)
    totals = jnp.sum(weights, axis=-1, keepdims=True)
    return highest, totals, dot(weights.astype(jnp.bfloat16), values[...])


def attention_near_body(q_ref, a_ref, acc_ref, stat_ref, padded_ref, keys, values):
    load_keys(a_ref, keys, values)
    for n in range(4):
        q = load_query(q_ref, n)
        padded_ref[n] = q
        highest, totals, out = attend(q, keys, values)
        acc_ref[n] = out
        stat_ref[n] = jnp.concatenate([highest + jnp.zeros_like(out), totals + jnp.zeros_like(out)], axis=1)


def attention_far_body(at_ref, q_ref, b_ref, acc_ref, stat_ref, o_ref, keys, values):
    quad = at_ref[2]
    load_keys(b_ref, keys, values)
    for n in range(4):
        highest, totals, out = attend(q_ref[n], keys, values)
        before, sums = stat_ref[n, :, 0:128], stat_ref[n, :, 128:256]
        top = jnp.maximum(highest, before)
        old = jnp.exp2((before - top) * score_scale)
        new = jnp.exp2((highest - top) * score_scale)
        out = (acc_ref[n] * old + out * new) / (sums * old + totals * new)
        o_ref[(quad + 4 - n) % 4] = out.astype(jnp.bfloat16)


def project_body(
    at_ref,
    att_ref,
    w0,
    w1,
    w2,
    w3,
    s1,
    s2,
    s3,
    w4,
    s4,
    res_ref,
    gain_ref,
    meta_ref,
    stream_ref,
    out_ref,
    rows,
):
    tp, core = at_ref[0], at_ref[1]
    turn = 1 - 2 * core

    def head(k):
        spot = (tp + 8 + k) % 8
        parts = [att_ref[8 * seq + spot].astype(jnp.float32) for seq in range(SEQS)]
        return jnp.concatenate(parts, axis=0)

    last = head(4)
    last = jnp.where(core == 0, last, pltpu.roll(last, 64, 1))
    lhs = [head(0), last]
    for k in (1, 2, 3):
        lhs += [head(-turn * k), head(turn * k)]
    lhs = jnp.concatenate(lhs, axis=1).astype(jnp.bfloat16)
    count = lhs.shape[0]
    row = lax.broadcasted_iota(jnp.int32, (count, count), 0)
    col = lax.broadcasted_iota(jnp.int32, (count, count), 1)
    turned = (col == row % SEQS * (count // SEQS) + row // SEQS).astype(jnp.bfloat16)
    lhs = dot(turned, lhs).astype(jnp.bfloat16)
    projected = dot(lhs[:, 0:256], jnp.concatenate([w0[...], w4[...], s4[...]], axis=0))
    for n, w_ref, s_ref in ((1, w1, s1), (2, w2, s2), (3, w3, s3)):
        both = jnp.concatenate([w_ref[...], s_ref[...]], axis=0)
        projected += dot(lhs[:, n * 256 : (n + 1) * 256], both)
    stream = (res_ref[...].astype(jnp.float32) + projected).astype(jnp.bfloat16)
    stream_ref[...] = stream
    wide = stream.astype(jnp.float32)
    normed = (
        wide * lax.rsqrt(jnp.mean(wide * wide, axis=-1, keepdims=True) + epsilon) * gain_ref[...]
    ).astype(jnp.bfloat16)
    first, second, before = places(meta_ref[...])
    both = first + second
    for slot in range(2):
        pick = (both * (before == slot).astype(jnp.float32)).T.astype(jnp.bfloat16)
        rows[slot * 128 : (slot + 1) * 128, :] = dot(pick, normed).astype(jnp.bfloat16)
    perm = packing(False)
    for b in range(8):
        out_ref[b * 256 : (b + 1) * 256, :] = pack_block(rows, b, perm)


def expert_body(at_ref, own_ref, got_ref, gate_ref, up_ref, down_ref, out_ref, rows):
    core = at_ref[1]
    unpack_rows(own_ref, got_ref, core, rows, packing(True))
    x = rows[...]
    hid = []
    for n in range(0, gate_ref.shape[1], 256):
        gate = dot(x, gate_ref[:, n : n + 256])
        up = dot(x, up_ref[:, n : n + 256])
        hidden = (gate / (1.0 + jnp.exp(-gate)) * up).astype(jnp.bfloat16)
        hid.append(hidden)
    hidden = jnp.concatenate(hid, axis=1)
    for n in range(0, D, 512):
        rows[:, n : n + 512] = dot(hidden, down_ref[:, n : n + 512]).astype(jnp.bfloat16)
    perm = packing(False)
    for b in range(8):
        side = core if b < 4 else 1 - core
        block = pack_block(rows, b, perm).reshape(16, 16, LANE)
        out_ref[b % 4 * 16 : (b % 4 + 1) * 16, half_of(side), :] = block


def combine_body(at_ref, own_ref, got_ref, stream_ref, meta_ref, out_ref, rows):
    core = at_ref[1]
    unpack_rows(own_ref, got_ref, core, rows, packing(True))
    meta = meta_ref[...]
    spot = meta[:, 0:2].astype(jnp.int32)
    spot = (spot >> 1) + 64 * ((spot & 1) ^ core)
    first, second, before = places(spot.astype(jnp.float32))
    logits = meta[:, 2:4]
    weights = jnp.exp(logits - jnp.max(logits, axis=-1, keepdims=True))
    mixing = weights / jnp.sum(weights, axis=-1, keepdims=True) * meta[:, 4:5]
    slots = [(before == slot).astype(jnp.float32) for slot in range(2)]
    total = stream_ref[...].astype(jnp.float32)
    r = rows[...]
    added = None
    for k, hot in enumerate((first, second)):
        pick = jnp.concatenate([hot * slots[0], hot * slots[1]], axis=-1).astype(jnp.bfloat16)
        term = dot(pick, r) * mixing[:, k : k + 1]
        added = term if added is None else added + term
    total = (total + added).astype(jnp.bfloat16)
    for p in range(out_ref.shape[0]):
        out_ref[p] = total[SEQS * p : SEQS * (p + 1), :]


def meta_body(route_ref, logit_ref, prob_ref, out_ref):
    rows = out_ref.shape[0]
    count = rows // SEQS
    row = lax.broadcasted_iota(jnp.int32, (rows, count), 0)
    col = lax.broadcasted_iota(jnp.int32, (rows, count), 1)
    total = None
    for seq in range(SEQS):
        e = route_ref[seq]
        e = (e >> 4) * 16 + (e & 7) * 2 + ((e >> 3) & 1)
        block = jnp.concatenate(
            [
                e.astype(jnp.float32),
                logit_ref[seq],
                prob_ref[seq : seq + 1, :],
                jnp.zeros((3, count), jnp.float32),
            ],
            axis=0,
        )
        part = lax.dot_general(
            (row == col * SEQS + seq).astype(jnp.float32),
            block,
            (((1,), (1,)), ((), ())),
            precision=lax.Precision.HIGHEST,
            preferred_element_type=jnp.float32,
        )
        total = part if total is None else total + part
    out_ref[...] = total


def vmem(*shape):
    return pltpu.VMEM(shape, jnp.bfloat16)


def params(mib):
    return pltpu.CompilerParams(vmem_limit_bytes=mib * 1024 * 1024)


def kernel_call(body, limit, **options):
    return pl.pallas_call(body, compiler_params=params(limit), **options)


VM = pl.BlockSpec(memory_space=pltpu.VMEM)
SM = pl.BlockSpec(memory_space=pltpu.SMEM)


def layer(
    residual,
    query,
    latent,
    rope_key,
    latent_gain,
    key_up,
    value_up,
    out_weight,
    norm_gain,
    group_prob,
    pair_logits,
    routes,
    w_gate,
    w_up,
    w_down,
):
    tp = lax.axis_index("tp")
    core = lax.axis_index("core")
    block = query.shape[0]
    rows = residual.shape[0] * SEQS
    tp_size = lax.axis_size("tp")
    quad = lax.axis_index("quad")
    at = jnp.stack([tp, core, quad]).astype(jnp.int32)

    spot = (lax.axis_index("half") * 4 + lax.axis_index("quad")) * 2 + core
    positions = spot * block + jnp.arange(block, dtype=jnp.int32)
    q = jnp.swapaxes(query, 0, 1)
    q_rot = rotate(q[..., NOPE:].astype(jnp.float32), positions).astype(jnp.bfloat16)
    q_rot = jnp.concatenate([q_rot[:, : block // 2], q_rot[:, block // 2 :]], axis=-1)
    q = jnp.concatenate([q[..., :NOPE], q_rot], axis=1)
    res = residual.reshape(rows, D)
    meta = kernel_call(
        meta_body,
        limit=2,
        out_shape=jax.ShapeDtypeStruct((rows, 8), jnp.float32),
        in_specs=[VM] * 3,
        out_specs=VM,
    )(jnp.transpose(routes, (1, 2, 0)), jnp.transpose(pair_logits, (1, 2, 0)), group_prob.T)
    q, res = lax.optimization_barrier((q, res))
    queries = []
    for k in range(4):
        piece = lax.dynamic_index_in_dim(q, (quad + k) % 4, 0, keepdims=False)
        queries.append(shift(piece, "quad", k, 4))
    queries = jnp.concatenate(queries, axis=0)

    lat = jnp.swapaxes(latent, 0, 1).astype(jnp.float32)
    lat = (
        lat * lax.rsqrt(jnp.mean(lat * lat, axis=-1, keepdims=True) + epsilon) * latent_gain
    ).astype(jnp.bfloat16)
    keys = jnp.einsum("spd,dc->spc", lat, key_up, preferred_element_type=jnp.float32)
    vals = jnp.einsum("spd,dc->spc", lat, value_up, preferred_element_type=jnp.float32)
    rot = rotate(jnp.swapaxes(rope_key, 0, 1).astype(jnp.float32), positions)
    rot = jnp.concatenate([rot[:, : block // 2], rot[:, block // 2 :]], axis=-1)
    kv = jnp.concatenate([keys, vals, rot], axis=1).astype(jnp.bfloat16)
    kv = jnp.concatenate([kv, kv], axis=0)
    kv, at = lax.optimization_barrier((kv, at))
    half_rows = out_weight.shape[0] // 2
    one, two = spread(out_weight, 1, tp_size), spread(out_weight, 2, tp_size)
    three = spread(two, 1, tp_size)
    part = lax.dynamic_slice(two, (core * half_rows, 0), (half_rows, D))
    four = spread(part, 2, tp_size)
    weights = [out_weight, one, two, three, swap(one), swap(two)]
    weights += [swap(three), four, swap(four)]

    near = lax.all_to_all(kv, Y, split_axis=0, concat_axis=0, tiled=True)
    far = swap(near)

    scratch = [vmem(8 * block, 256), vmem(8 * block, VDIM)]
    partial, stats, padded = kernel_call(
        attention_near_body,
        limit=12,
        out_shape=(
            jax.ShapeDtypeStruct((4, block, VDIM), jnp.float32),
            jax.ShapeDtypeStruct((4, block, 2 * VDIM), jnp.float32),
            jax.ShapeDtypeStruct((4, block, 256), jnp.bfloat16),
        ),
        in_specs=[VM] * 2,
        out_specs=(VM, VM, VM),
        scratch_shapes=scratch,
    )(queries, near)
    attended = kernel_call(
        attention_far_body,
        limit=12,
        out_shape=jax.ShapeDtypeStruct((4, block, VDIM), jnp.bfloat16),
        in_specs=[SM] + [VM] * 4,
        out_specs=VM,
        scratch_shapes=scratch,
    )(at, padded, far, partial, stats)
    attended = attended.reshape(4 * tp_size, block // tp_size, VDIM)
    attended = lax.all_to_all(attended, ("quad", "tp"), split_axis=0, concat_axis=0, tiled=True)

    stream, outgoing = kernel_call(
        project_body,
        limit=10,
        out_shape=(
            jax.ShapeDtypeStruct((rows, D), jnp.bfloat16),
            jax.ShapeDtypeStruct((2048, LANE), jnp.bfloat16),
        ),
        in_specs=[SM] + [VM] * 13,
        out_specs=(VM, VM),
        scratch_shapes=[vmem(256, D)],
    )(at, attended, *weights, res, norm_gain.reshape(1, D), meta)

    def exchange(x):
        own = lax.all_to_all(
            x.reshape(64, 32, LANE), PLANE, split_axis=0, concat_axis=0, tiled=True
        )
        other = kernel_call(
            pick_body,
            limit=2,
            out_shape=jax.ShapeDtypeStruct((64, 16, LANE), jnp.bfloat16),
            in_specs=[SM, VM],
            out_specs=VM,
        )(at, own)
        return own, swap(other)

    served = kernel_call(
        expert_body,
        limit=10,
        out_shape=jax.ShapeDtypeStruct((64, 32, LANE), jnp.bfloat16),
        in_specs=[SM] + [VM] * 5,
        out_specs=VM,
        scratch_shapes=[vmem(256, D)],
    )(at, *exchange(outgoing), w_gate[0], w_up[0], w_down[0])
    combined = kernel_call(
        combine_body,
        limit=8,
        out_shape=jax.ShapeDtypeStruct(residual.shape, jnp.bfloat16),
        in_specs=[SM] + [VM] * 4,
        out_specs=VM,
        scratch_shapes=[vmem(256, D)],
    )(at, *exchange(served), stream, meta)
    return combined


def solution(mesh):
    shape = mesh.shape
    devices = np.asarray(mesh.devices).reshape(
        shape["grp"], 2, 4, shape["sp"] // 8, shape["tp"]
    )
    fine = Mesh(devices, ("grp", "half", "quad", "core", "tp"))
    sp = ("half", "quad", "core")
    both = ("half", "quad", "core", "tp")
    placed = (
        P(both, "grp", None),
        P(sp, "grp", "tp"),
        P(sp, "grp", None),
        P(sp, "grp", None),
        P(),
        P(None, "tp"),
        P(None, "tp"),
        P("tp", None),
        P(),
        P(both, "grp"),
        P(both, "grp", None),
        P(both, "grp", None),
        P(both, None, None),
        P(both, None, None),
        P(both, None, None),
    )
    return jax.shard_map(
        layer, mesh=fine, in_specs=placed, out_specs=P(both, "grp", None), check_vma=False
    )
```

```python
import jax
import jax.numpy as jnp
import numpy as np
from jax import lax
from jax.experimental import pallas as pl
from jax.experimental.pallas import tpu as pltpu
from jax.sharding import Mesh, PartitionSpec as P


D = 2048
NOPE = 128
ROPE = 64
VDIM = 128
QK = 192
SEQS = 4
CHIPS = 8
LANE = 256
BANDS = D // LANE

epsilon = 1e-06
rotary_base = 10000.0
score_scale = QK ** (-0.5) * 1.4426950408889634

Y = ("half", "quad")
ALL = ("half", "quad", "core", "tp")


def rotate(values, positions):
    halfway = values.shape[-1] // 2
    inverse = rotary_base ** (-jnp.arange(halfway, dtype=jnp.float32) / halfway)
    angles = positions.astype(jnp.float32)[:, None] * inverse[None, :]
    angles = angles.reshape((1, angles.shape[0], halfway))
    cosine_values = jnp.cos(angles)
    sine_values = jnp.sin(angles)
    first_half = values[..., :halfway]
    second_half = values[..., halfway:]
    return jnp.concatenate(
        [
            first_half * cosine_values - second_half * sine_values,
            second_half * cosine_values + first_half * sine_values,
        ],
        axis=-1,
    )


def shift(x, axis, by, size):
    if by == 0:
        return x
    return lax.ppermute(x, axis, [(i, (i + by) % size) for i in range(size)])


def swap(x):
    return lax.ppermute(x, "core", [(0, 1), (1, 0)])


def spread(x, by, size):
    pairs = []
    for i in range(size):
        pairs.append((i, (i + by) % size))
        pairs.append((size + i, size + (i - by) % size))
    return lax.ppermute(x, ("core", "tp"), pairs)


def dot(a, b):
    return lax.dot_general(a, b, (((1,), (0,)), ((), ())), preferred_element_type=jnp.float32)


def packing(inverse):
    i = lax.broadcasted_iota(jnp.int32, (256, 256), 1 if inverse else 0)
    k = lax.broadcasted_iota(jnp.int32, (256, 256), 0 if inverse else 1)
    d, r = i // 16, i % 16
    return (k == (r // 2) * 32 + (r % 2) * 16 + d).astype(jnp.bfloat16)


def pack_rows(rows_ref, out_ref, perm):
    for b in range(8):
        stack = []
        for j in range(BANDS):
            for slot in range(2):
                lo = slot * 128 + b * 16
                stack.append(rows_ref[lo : lo + 16, j * LANE : (j + 1) * LANE])
        out_ref[b * 256 : (b + 1) * 256, :] = dot(perm, jnp.concatenate(stack, axis=0)).astype(
            jnp.bfloat16
        )


def unpack_rows(in_ref, rows_ref, perm):
    for b in range(8):
        block = dot(perm, in_ref[b * 256 : (b + 1) * 256, :]).astype(jnp.bfloat16)
        for j in range(BANDS):
            for slot in range(2):
                lo = slot * 128 + b * 16
                at = j * 32 + slot * 16
                rows_ref[lo : lo + 16, j * LANE : (j + 1) * LANE] = block[at : at + 16, :]


def places(meta):
    rows = meta.shape[0]
    expert = lax.broadcasted_iota(jnp.int32, (rows, 128), 1).astype(jnp.float32)
    first = (meta[:, 0:1] == expert).astype(jnp.float32)
    second = (meta[:, 1:2] == expert).astype(jnp.float32)
    earlier = (
        lax.broadcasted_iota(jnp.int32, (rows, rows), 0)
        > lax.broadcasted_iota(jnp.int32, (rows, rows), 1)
    ).astype(jnp.bfloat16)
    before = dot(earlier, (first + second).astype(jnp.bfloat16))
    return first, second, before


def expand_body(lat_ref, rope_ref, turn_ref, gain_ref, key_ref, value_ref, out_ref):
    block = lat_ref.shape[1]
    half = block // 2
    turn = turn_ref[...]
    for s in range(SEQS):
        lat = lat_ref[s].astype(jnp.float32)
        scale = lax.rsqrt(jnp.mean(lat * lat, axis=-1, keepdims=True) + epsilon)
        lat = (lat * scale * gain_ref[...]).astype(jnp.bfloat16)
        keys = dot(lat, key_ref[...]).astype(jnp.bfloat16)
        values = dot(lat, value_ref[...]).astype(jnp.bfloat16)
        rope = rope_ref[s].astype(jnp.float32)
        rope = jnp.concatenate([rope, rope], axis=1)
        rot = rope * turn[:, 0:128] + pltpu.roll(rope, 32, 1) * turn[:, 128:256]
        low = lax.broadcasted_iota(jnp.int32, (half, 128), 1) < ROPE
        rot = jnp.where(low, rot[0:half], rot[half:]).astype(jnp.bfloat16)
        for at in (s, SEQS + s):
            out_ref[at, 0:block, :] = keys
            out_ref[at, block : 2 * block, :] = values
            out_ref[at, 2 * block :, :] = rot


def load_keys(src, keys, values):
    for j in range(8):
        lo, hi = j * 96, 768 + j * 96
        keys[lo : lo + 96, 0:128] = src[j, 0:96, :]
        keys[hi : hi + 96, 0:128] = src[j, 96:192, :]
        values[lo : lo + 96, :] = src[j, 192:288, :]
        values[hi : hi + 96, :] = src[j, 288:384, :]
        rot = src[j, 384:480, :]
        keys[lo : lo + 96, 128:256] = rot
        keys[hi : hi + 96, 128:256] = pltpu.roll(rot.astype(jnp.float32), 64, 1).astype(
            jnp.bfloat16
        )


def load_query(q_ref, n):
    base = n * 288
    rot = q_ref[base + 192 : base + 288, :].astype(jnp.float32)
    low = lax.broadcasted_iota(jnp.int32, rot.shape, 1) < ROPE
    first = jnp.where(low, rot, 0.0).astype(jnp.bfloat16)
    second = jnp.where(low, pltpu.roll(rot, 64, 1), 0.0).astype(jnp.bfloat16)
    rot = jnp.concatenate([first, second], axis=0)
    return jnp.concatenate([q_ref[base : base + 192, :], rot], axis=1)


def attend(q, keys, values):
    scores = lax.dot_general(
        q, keys[...], (((1,), (1,)), ((), ())), preferred_element_type=jnp.float32
    )
    highest = jnp.max(scores, axis=-1, keepdims=True)
    weights = jnp.exp2((scores - highest) * score_scale)
    totals = jnp.sum(weights, axis=-1, keepdims=True)
    return highest, totals, dot(weights.astype(jnp.bfloat16), values[...])


def attention_near_body(q_ref, a_ref, acc_ref, stat_ref, padded_ref, keys, values):
    load_keys(a_ref, keys, values)
    for n in range(4):
        q = load_query(q_ref, n)
        padded_ref[n] = q
        highest, totals, out = attend(q, keys, values)
        acc_ref[n] = out
        stat_ref[n] = jnp.concatenate([highest + jnp.zeros_like(out), totals + jnp.zeros_like(out)], axis=1)


def attention_far_body(at_ref, q_ref, b_ref, acc_ref, stat_ref, o_ref, keys, values):
    quad = at_ref[2]
    load_keys(b_ref, keys, values)
    for n in range(4):
        highest, totals, out = attend(q_ref[n], keys, values)
        before, sums = stat_ref[n, :, 0:128], stat_ref[n, :, 128:256]
        top = jnp.maximum(highest, before)
        old = jnp.exp2((before - top) * score_scale)
        new = jnp.exp2((highest - top) * score_scale)
        out = (acc_ref[n] * old + out * new) / (sums * old + totals * new)
        o_ref[(quad + 4 - n) % 4] = out.astype(jnp.bfloat16)


def project_body(
    at_ref,
    att_ref,
    w0,
    w1,
    w2,
    w3,
    s1,
    s2,
    s3,
    w4,
    s4,
    res_ref,
    gain_ref,
    meta_ref,
    stream_ref,
    out_ref,
    rows,
):
    tp, core = at_ref[0], at_ref[1]
    turn = 1 - 2 * core

    def head(k):
        spot = (tp + 8 + k) % 8
        parts = [att_ref[8 * seq + spot].astype(jnp.float32) for seq in range(SEQS)]
        return jnp.concatenate(parts, axis=0)

    last = head(4)
    last = jnp.where(core == 0, last, pltpu.roll(last, 64, 1))
    lhs = [head(0), last]
    for k in (1, 2, 3):
        lhs += [head(-turn * k), head(turn * k)]
    lhs = jnp.concatenate(lhs, axis=1).astype(jnp.bfloat16)
    count = lhs.shape[0]
    row = lax.broadcasted_iota(jnp.int32, (count, count), 0)
    col = lax.broadcasted_iota(jnp.int32, (count, count), 1)
    turned = (col == row % SEQS * (count // SEQS) + row // SEQS).astype(jnp.bfloat16)
    lhs = dot(turned, lhs).astype(jnp.bfloat16)
    projected = dot(lhs[:, 0:256], jnp.concatenate([w0[...], w4[...], s4[...]], axis=0))
    for n, w_ref, s_ref in ((1, w1, s1), (2, w2, s2), (3, w3, s3)):
        both = jnp.concatenate([w_ref[...], s_ref[...]], axis=0)
        projected += dot(lhs[:, n * 256 : (n + 1) * 256], both)
    stream = (res_ref[...].astype(jnp.float32) + projected).astype(jnp.bfloat16)
    stream_ref[...] = stream
    wide = stream.astype(jnp.float32)
    normed = (
        wide * lax.rsqrt(jnp.mean(wide * wide, axis=-1, keepdims=True) + epsilon) * gain_ref[...]
    ).astype(jnp.bfloat16)
    first, second, before = places(meta_ref[...])
    both = first + second
    for slot in range(2):
        pick = (both * (before == slot).astype(jnp.float32)).T.astype(jnp.bfloat16)
        rows[slot * 128 : (slot + 1) * 128, :] = dot(pick, normed).astype(jnp.bfloat16)
    pack_rows(rows, out_ref, packing(False))


def expert_body(in_ref, gate_ref, up_ref, down_ref, out_ref, rows):
    unpack_rows(in_ref, rows, packing(True))
    x = rows[...]
    hid = []
    for n in range(0, gate_ref.shape[1], 256):
        gate = dot(x, gate_ref[:, n : n + 256])
        up = dot(x, up_ref[:, n : n + 256])
        hidden = (gate / (1.0 + jnp.exp(-gate)) * up).astype(jnp.bfloat16)
        hid.append(hidden)
    hidden = jnp.concatenate(hid, axis=1)
    for n in range(0, D, 512):
        rows[:, n : n + 512] = dot(hidden, down_ref[:, n : n + 512]).astype(jnp.bfloat16)
    pack_rows(rows, out_ref, packing(False))


def combine_body(in_ref, stream_ref, meta_ref, out_ref, rows):
    unpack_rows(in_ref, rows, packing(True))
    meta = meta_ref[...]
    first, second, before = places(meta)
    logits = meta[:, 2:4]
    weights = jnp.exp(logits - jnp.max(logits, axis=-1, keepdims=True))
    mixing = weights / jnp.sum(weights, axis=-1, keepdims=True) * meta[:, 4:5]
    slots = [(before == slot).astype(jnp.float32) for slot in range(2)]
    total = stream_ref[...].astype(jnp.float32)
    r = rows[...]
    added = None
    for k, hot in enumerate((first, second)):
        pick = jnp.concatenate([hot * slots[0], hot * slots[1]], axis=-1).astype(jnp.bfloat16)
        term = dot(pick, r) * mixing[:, k : k + 1]
        added = term if added is None else added + term
    total = (total + added).astype(jnp.bfloat16)
    for p in range(out_ref.shape[0]):
        out_ref[p] = total[SEQS * p : SEQS * (p + 1), :]


def meta_body(route_ref, logit_ref, prob_ref, out_ref):
    rows = out_ref.shape[0]
    count = rows // SEQS
    row = lax.broadcasted_iota(jnp.int32, (rows, count), 0)
    col = lax.broadcasted_iota(jnp.int32, (rows, count), 1)
    total = None
    for seq in range(SEQS):
        block = jnp.concatenate(
            [
                route_ref[seq].astype(jnp.float32),
                logit_ref[seq],
                prob_ref[seq : seq + 1, :],
                jnp.zeros((3, count), jnp.float32),
            ],
            axis=0,
        )
        part = lax.dot_general(
            (row == col * SEQS + seq).astype(jnp.float32),
            block,
            (((1,), (1,)), ((), ())),
            precision=lax.Precision.HIGHEST,
            preferred_element_type=jnp.float32,
        )
        total = part if total is None else total + part
    out_ref[...] = total


def vmem(*shape):
    return pltpu.VMEM(shape, jnp.bfloat16)


def params(mib):
    return pltpu.CompilerParams(vmem_limit_bytes=mib * 1024 * 1024)


def kernel_call(body, limit, **options):
    return pl.pallas_call(body, compiler_params=params(limit), **options)


VM = pl.BlockSpec(memory_space=pltpu.VMEM)
SM = pl.BlockSpec(memory_space=pltpu.SMEM)


def layer(
    residual,
    query,
    latent,
    rope_key,
    latent_gain,
    key_up,
    value_up,
    out_weight,
    norm_gain,
    group_prob,
    pair_logits,
    routes,
    w_gate,
    w_up,
    w_down,
):
    tp = lax.axis_index("tp")
    core = lax.axis_index("core")
    block = query.shape[0]
    rows = residual.shape[0] * SEQS
    tp_size = lax.axis_size("tp")
    quad = lax.axis_index("quad")
    at = jnp.stack([tp, core, quad]).astype(jnp.int32)

    spot = (lax.axis_index("half") * 4 + lax.axis_index("quad")) * 2 + core
    positions = spot * block + jnp.arange(block, dtype=jnp.int32)
    q = jnp.swapaxes(query, 0, 1)
    q_rot = rotate(q[..., NOPE:].astype(jnp.float32), positions).astype(jnp.bfloat16)
    q_rot = jnp.concatenate([q_rot[:, : block // 2], q_rot[:, block // 2 :]], axis=-1)
    q = jnp.concatenate([q[..., :NOPE], q_rot], axis=1)
    res = residual.reshape(rows, D)
    meta = kernel_call(
        meta_body,
        limit=2,
        out_shape=jax.ShapeDtypeStruct((rows, 8), jnp.float32),
        in_specs=[VM] * 3,
        out_specs=VM,
    )(jnp.transpose(routes, (1, 2, 0)), jnp.transpose(pair_logits, (1, 2, 0)), group_prob.T)
    q, res = lax.optimization_barrier((q, res))
    queries = []
    for k in range(4):
        piece = lax.dynamic_index_in_dim(q, (quad + k) % 4, 0, keepdims=False)
        queries.append(shift(piece, "quad", k, 4))
    queries = jnp.concatenate(queries, axis=0)

    halfway = ROPE // 2
    inverse = rotary_base ** (-jnp.arange(halfway, dtype=jnp.float32) / halfway)
    angles = positions.astype(jnp.float32)[:, None] * jnp.concatenate([inverse] * 4)[None, :]
    sign = jnp.concatenate([-jnp.ones((halfway,)), jnp.ones((halfway,))] * 2)[None, :]
    turn = jnp.concatenate([jnp.cos(angles), jnp.sin(angles) * sign], axis=1)
    kv = kernel_call(
        expand_body,
        limit=12,
        out_shape=jax.ShapeDtypeStruct((CHIPS, 2 * block + block // 2, 128), jnp.bfloat16),
        in_specs=[VM] * 6,
        out_specs=VM,
    )(
        jnp.swapaxes(latent, 0, 1),
        jnp.swapaxes(rope_key, 0, 1),
        turn,
        latent_gain.reshape(1, -1),
        key_up,
        value_up,
    )
    kv, at = lax.optimization_barrier((kv, at))
    half_rows = out_weight.shape[0] // 2
    one, two = spread(out_weight, 1, tp_size), spread(out_weight, 2, tp_size)
    three = spread(two, 1, tp_size)
    part = lax.dynamic_slice(two, (core * half_rows, 0), (half_rows, D))
    four = spread(part, 2, tp_size)
    weights = [out_weight, one, two, three, swap(one), swap(two)]
    weights += [swap(three), four, swap(four)]

    near = lax.all_to_all(kv, Y, split_axis=0, concat_axis=0, tiled=True)
    far = swap(near)

    scratch = [vmem(8 * block, 256), vmem(8 * block, VDIM)]
    partial, stats, padded = kernel_call(
        attention_near_body,
        limit=12,
        out_shape=(
            jax.ShapeDtypeStruct((4, block, VDIM), jnp.float32),
            jax.ShapeDtypeStruct((4, block, 2 * VDIM), jnp.float32),
            jax.ShapeDtypeStruct((4, block, 256), jnp.bfloat16),
        ),
        in_specs=[VM] * 2,
        out_specs=(VM, VM, VM),
        scratch_shapes=scratch,
    )(queries, near)
    attended = kernel_call(
        attention_far_body,
        limit=12,
        out_shape=jax.ShapeDtypeStruct((4, block, VDIM), jnp.bfloat16),
        in_specs=[SM] + [VM] * 4,
        out_specs=VM,
        scratch_shapes=scratch,
    )(at, padded, far, partial, stats)
    attended = attended.reshape(4 * tp_size, block // tp_size, VDIM)
    attended = lax.all_to_all(attended, ("quad", "tp"), split_axis=0, concat_axis=0, tiled=True)

    stream, outgoing = kernel_call(
        project_body,
        limit=10,
        out_shape=(
            jax.ShapeDtypeStruct((rows, D), jnp.bfloat16),
            jax.ShapeDtypeStruct((2048, LANE), jnp.bfloat16),
        ),
        in_specs=[SM] + [VM] * 13,
        out_specs=(VM, VM),
        scratch_shapes=[vmem(256, D)],
    )(at, attended, *weights, res, norm_gain.reshape(1, D), meta)

    def exchange(x):
        x = x.reshape(128, 16, LANE)
        return lax.all_to_all(x, ALL, split_axis=0, concat_axis=0, tiled=True).reshape(2048, LANE)

    arrived = exchange(outgoing)
    served = kernel_call(
        expert_body,
        limit=10,
        out_shape=jax.ShapeDtypeStruct((2048, LANE), jnp.bfloat16),
        in_specs=[VM] * 4,
        out_specs=VM,
        scratch_shapes=[vmem(256, D)],
    )(arrived, w_gate[0], w_up[0], w_down[0])
    returned = exchange(served)
    combined = kernel_call(
        combine_body,
        limit=8,
        out_shape=jax.ShapeDtypeStruct(residual.shape, jnp.bfloat16),
        in_specs=[VM] * 3,
        out_specs=VM,
        scratch_shapes=[vmem(256, D)],
    )(returned, stream, meta)
    return combined


def solution(mesh):
    shape = mesh.shape
    devices = np.asarray(mesh.devices).reshape(
        shape["grp"], 2, 4, shape["sp"] // 8, shape["tp"]
    )
    fine = Mesh(devices, ("grp", "half", "quad", "core", "tp"))
    sp = ("half", "quad", "core")
    both = ("half", "quad", "core", "tp")
    placed = (
        P(both, "grp", None),
        P(sp, "grp", "tp"),
        P(sp, "grp", None),
        P(sp, "grp", None),
        P(),
        P(None, "tp"),
        P(None, "tp"),
        P("tp", None),
        P(),
        P(both, "grp"),
        P(both, "grp", None),
        P(both, "grp", None),
        P(both, None, None),
        P(both, None, None),
        P(both, None, None),
    )
    return jax.shard_map(
        layer, mesh=fine, in_specs=placed, out_specs=P(both, "grp", None), check_vma=False
    )
```

```python
import jax
import jax.numpy as jnp
import numpy as np
from jax import lax
from jax.experimental import pallas as pl
from jax.experimental.pallas import tpu as pltpu
from jax.sharding import Mesh, PartitionSpec as P


D = 2048
NOPE = 128
ROPE = 64
VDIM = 128
QK = 192
SEQS = 4
LANE = 256
BANDS = D // LANE

epsilon = 1e-06
rotary_base = 10000.0
score_scale = QK ** (-0.5) * 1.4426950408889634

Y = ("half", "quad")
ALL = ("half", "quad", "core", "tp")


def rotate(values, positions):
    halfway = values.shape[-1] // 2
    inverse = rotary_base ** (-jnp.arange(halfway, dtype=jnp.float32) / halfway)
    angles = positions.astype(jnp.float32)[:, None] * inverse[None, :]
    angles = angles.reshape((1, angles.shape[0], halfway))
    cosine_values = jnp.cos(angles)
    sine_values = jnp.sin(angles)
    first_half = values[..., :halfway]
    second_half = values[..., halfway:]
    return jnp.concatenate(
        [
            first_half * cosine_values - second_half * sine_values,
            second_half * cosine_values + first_half * sine_values,
        ],
        axis=-1,
    )


def shift(x, axis, by, size):
    if by == 0:
        return x
    return lax.ppermute(x, axis, [(i, (i + by) % size) for i in range(size)])


def swap(x):
    return lax.ppermute(x, "core", [(0, 1), (1, 0)])


def spread(x, by, size):
    pairs = []
    for i in range(size):
        pairs.append((i, (i + by) % size))
        pairs.append((size + i, size + (i - by) % size))
    return lax.ppermute(x, ("core", "tp"), pairs)


def dot(a, b):
    return lax.dot_general(a, b, (((1,), (0,)), ((), ())), preferred_element_type=jnp.float32)


def packing(inverse):
    i = lax.broadcasted_iota(jnp.int32, (256, 256), 1 if inverse else 0)
    k = lax.broadcasted_iota(jnp.int32, (256, 256), 0 if inverse else 1)
    d, r = i // 16, i % 16
    return (k == (r // 2) * 32 + (r % 2) * 16 + d).astype(jnp.bfloat16)


def pack_rows(rows_ref, out_ref, perm):
    for b in range(8):
        stack = []
        for j in range(BANDS):
            for slot in range(2):
                lo = slot * 128 + b * 16
                stack.append(rows_ref[lo : lo + 16, j * LANE : (j + 1) * LANE])
        out_ref[b * 256 : (b + 1) * 256, :] = dot(perm, jnp.concatenate(stack, axis=0)).astype(
            jnp.bfloat16
        )


def unpack_rows(in_ref, rows_ref, perm):
    for b in range(8):
        block = dot(perm, in_ref[b * 256 : (b + 1) * 256, :]).astype(jnp.bfloat16)
        for j in range(BANDS):
            for slot in range(2):
                lo = slot * 128 + b * 16
                at = j * 32 + slot * 16
                rows_ref[lo : lo + 16, j * LANE : (j + 1) * LANE] = block[at : at + 16, :]


def places(meta):
    rows = meta.shape[0]
    expert = lax.broadcasted_iota(jnp.int32, (rows, 128), 1).astype(jnp.float32)
    first = (meta[:, 0:1] == expert).astype(jnp.float32)
    second = (meta[:, 1:2] == expert).astype(jnp.float32)
    earlier = (
        lax.broadcasted_iota(jnp.int32, (rows, rows), 0)
        > lax.broadcasted_iota(jnp.int32, (rows, rows), 1)
    ).astype(jnp.bfloat16)
    before = dot(earlier, (first + second).astype(jnp.bfloat16))
    return first, second, before


def load_keys(src, keys, values):
    for j in range(8):
        lo, hi = j * 96, 768 + j * 96
        keys[lo : lo + 96, 0:128] = src[j, 0:96, :]
        keys[hi : hi + 96, 0:128] = src[j, 96:192, :]
        values[lo : lo + 96, :] = src[j, 192:288, :]
        values[hi : hi + 96, :] = src[j, 288:384, :]
        rot = src[j, 384:480, :]
        keys[lo : lo + 96, 128:256] = rot
        keys[hi : hi + 96, 128:256] = pltpu.roll(rot.astype(jnp.float32), 64, 1).astype(
            jnp.bfloat16
        )


def load_query(q_ref, n):
    base = n * 288
    rot = q_ref[base + 192 : base + 288, :].astype(jnp.float32)
    low = lax.broadcasted_iota(jnp.int32, rot.shape, 1) < ROPE
    first = jnp.where(low, rot, 0.0).astype(jnp.bfloat16)
    second = jnp.where(low, pltpu.roll(rot, 64, 1), 0.0).astype(jnp.bfloat16)
    rot = jnp.concatenate([first, second], axis=0)
    return jnp.concatenate([q_ref[base : base + 192, :], rot], axis=1)


def attend(q, keys, values):
    scores = lax.dot_general(
        q, keys[...], (((1,), (1,)), ((), ())), preferred_element_type=jnp.float32
    )
    highest = jnp.max(scores, axis=-1, keepdims=True)
    weights = jnp.exp2((scores - highest) * score_scale)
    totals = jnp.sum(weights, axis=-1, keepdims=True)
    return highest, totals, dot(weights.astype(jnp.bfloat16), values[...])


def attention_near_body(q_ref, a_ref, acc_ref, stat_ref, padded_ref, keys, values):
    load_keys(a_ref, keys, values)
    for n in range(4):
        q = load_query(q_ref, n)
        padded_ref[n] = q
        highest, totals, out = attend(q, keys, values)
        acc_ref[n] = out
        stat_ref[n] = jnp.concatenate([highest + jnp.zeros_like(out), totals + jnp.zeros_like(out)], axis=1)


def attention_far_body(at_ref, q_ref, b_ref, acc_ref, stat_ref, o_ref, keys, values):
    quad = at_ref[2]
    load_keys(b_ref, keys, values)
    for n in range(4):
        highest, totals, out = attend(q_ref[n], keys, values)
        before, sums = stat_ref[n, :, 0:128], stat_ref[n, :, 128:256]
        top = jnp.maximum(highest, before)
        old = jnp.exp2((before - top) * score_scale)
        new = jnp.exp2((highest - top) * score_scale)
        out = (acc_ref[n] * old + out * new) / (sums * old + totals * new)
        o_ref[(quad + 4 - n) % 4] = out.astype(jnp.bfloat16)


def project_body(
    at_ref,
    att_ref,
    w1,
    w2,
    w3,
    s1,
    s2,
    s3,
    w4,
    s4,
    res_ref,
    gain_ref,
    meta_ref,
    stream_ref,
    out_ref,
    rows,
):
    tp, core = at_ref[0], at_ref[1]
    turn = 1 - 2 * core

    def head(k):
        spot = (tp + 8 + k) % 8
        parts = [att_ref[8 * seq + spot].astype(jnp.float32) for seq in range(SEQS)]
        return jnp.concatenate(parts, axis=0)

    last = head(4)
    last = jnp.where(core == 0, last, pltpu.roll(last, 64, 1))
    lhs = [head(0), last]
    for k in (1, 2, 3):
        lhs += [head(-turn * k), head(turn * k)]
    lhs = jnp.concatenate(lhs, axis=1).astype(jnp.bfloat16)
    count = lhs.shape[0]
    row = lax.broadcasted_iota(jnp.int32, (count, count), 0)
    col = lax.broadcasted_iota(jnp.int32, (count, count), 1)
    turned = (col == row % SEQS * (count // SEQS) + row // SEQS).astype(jnp.bfloat16)
    lhs = dot(turned, lhs).astype(jnp.bfloat16)
    first = jnp.concatenate([res_ref[count:, :], w4[...], s4[...]], axis=0)
    projected = dot(lhs[:, 0:256], first)
    for n, w_ref, s_ref in ((1, w1, s1), (2, w2, s2), (3, w3, s3)):
        both = jnp.concatenate([w_ref[...], s_ref[...]], axis=0)
        projected += dot(lhs[:, n * 256 : (n + 1) * 256], both)
    stream = (res_ref[0:count, :].astype(jnp.float32) + projected).astype(jnp.bfloat16)
    stream_ref[...] = stream
    wide = stream.astype(jnp.float32)
    normed = (
        wide * lax.rsqrt(jnp.mean(wide * wide, axis=-1, keepdims=True) + epsilon) * gain_ref[...]
    ).astype(jnp.bfloat16)
    first, second, before = places(meta_ref[...])
    both = first + second
    for slot in range(2):
        pick = (both * (before == slot).astype(jnp.float32)).T.astype(jnp.bfloat16)
        rows[slot * 128 : (slot + 1) * 128, :] = dot(pick, normed).astype(jnp.bfloat16)
    pack_rows(rows, out_ref, packing(False))


def expert_body(in_ref, gate_ref, up_ref, down_ref, out_ref, rows):
    unpack_rows(in_ref, rows, packing(True))
    x = rows[...]
    hid = []
    for n in range(0, gate_ref.shape[1], 256):
        gate = dot(x, gate_ref[:, n : n + 256])
        up = dot(x, up_ref[:, n : n + 256])
        hidden = (gate / (1.0 + jnp.exp(-gate)) * up).astype(jnp.bfloat16)
        hid.append(hidden)
    hidden = jnp.concatenate(hid, axis=1)
    for n in range(0, D, 512):
        rows[:, n : n + 512] = dot(hidden, down_ref[:, n : n + 512]).astype(jnp.bfloat16)
    pack_rows(rows, out_ref, packing(False))


def combine_body(in_ref, stream_ref, meta_ref, out_ref, rows):
    unpack_rows(in_ref, rows, packing(True))
    meta = meta_ref[...]
    first, second, before = places(meta)
    logits = meta[:, 2:4]
    weights = jnp.exp(logits - jnp.max(logits, axis=-1, keepdims=True))
    mixing = weights / jnp.sum(weights, axis=-1, keepdims=True) * meta[:, 4:5]
    slots = [(before == slot).astype(jnp.float32) for slot in range(2)]
    total = stream_ref[...].astype(jnp.float32)
    r = rows[...]
    added = None
    for k, hot in enumerate((first, second)):
        pick = jnp.concatenate([hot * slots[0], hot * slots[1]], axis=-1).astype(jnp.bfloat16)
        term = dot(pick, r) * mixing[:, k : k + 1]
        added = term if added is None else added + term
    total = (total + added).astype(jnp.bfloat16)
    for p in range(out_ref.shape[0]):
        out_ref[p] = total[SEQS * p : SEQS * (p + 1), :]


def vmem(*shape):
    return pltpu.VMEM(shape, jnp.bfloat16)


def params(mib):
    return pltpu.CompilerParams(vmem_limit_bytes=mib * 1024 * 1024)


def kernel_call(body, limit, **options):
    return pl.pallas_call(body, compiler_params=params(limit), **options)


VM = pl.BlockSpec(memory_space=pltpu.VMEM)
SM = pl.BlockSpec(memory_space=pltpu.SMEM)


def layer(
    residual,
    query,
    latent,
    rope_key,
    latent_gain,
    key_up,
    value_up,
    out_weight,
    norm_gain,
    group_prob,
    pair_logits,
    routes,
    w_gate,
    w_up,
    w_down,
):
    tp = lax.axis_index("tp")
    core = lax.axis_index("core")
    block = query.shape[0]
    rows = residual.shape[0] * SEQS
    tp_size = lax.axis_size("tp")
    quad = lax.axis_index("quad")
    at = jnp.stack([tp, core, quad]).astype(jnp.int32)

    spot = (lax.axis_index("half") * 4 + lax.axis_index("quad")) * 2 + core
    positions = spot * block + jnp.arange(block, dtype=jnp.int32)
    q = jnp.swapaxes(query, 0, 1)
    q_rot = rotate(q[..., NOPE:].astype(jnp.float32), positions).astype(jnp.bfloat16)
    q_rot = jnp.concatenate([q_rot[:, : block // 2], q_rot[:, block // 2 :]], axis=-1)
    q = jnp.concatenate([q[..., :NOPE], q_rot], axis=1)
    res = jnp.concatenate([residual.reshape(rows, D), out_weight], axis=0)
    meta = jnp.concatenate(
        [routes.astype(jnp.float32), pair_logits, group_prob[..., None]], axis=-1
    )
    meta = meta.reshape(rows, 5)
    q, res, meta = lax.optimization_barrier((q, res, meta))
    queries = []
    for k in range(4):
        piece = lax.dynamic_index_in_dim(q, (quad + k) % 4, 0, keepdims=False)
        queries.append(shift(piece, "quad", k, 4))
    queries = jnp.concatenate(queries, axis=0)

    lat = jnp.swapaxes(latent, 0, 1).astype(jnp.float32)
    lat = (
        lat * lax.rsqrt(jnp.mean(lat * lat, axis=-1, keepdims=True) + epsilon) * latent_gain
    ).astype(jnp.bfloat16)
    keys = jnp.einsum("spd,dc->spc", lat, key_up, preferred_element_type=jnp.float32)
    vals = jnp.einsum("spd,dc->spc", lat, value_up, preferred_element_type=jnp.float32)
    rot = rotate(jnp.swapaxes(rope_key, 0, 1).astype(jnp.float32), positions)
    rot = jnp.concatenate([rot[:, : block // 2], rot[:, block // 2 :]], axis=-1)
    kv = jnp.concatenate([keys, vals, rot], axis=1).astype(jnp.bfloat16)
    kv = jnp.concatenate([kv, kv], axis=0)
    kv, at = lax.optimization_barrier((kv, at))
    half_rows = out_weight.shape[0] // 2
    one, two = spread(out_weight, 1, tp_size), spread(out_weight, 2, tp_size)
    three = spread(two, 1, tp_size)
    part = lax.dynamic_slice(two, (core * half_rows, 0), (half_rows, D))
    four = spread(part, 2, tp_size)
    weights = [one, two, three, swap(one), swap(two)]
    weights += [swap(three), four, swap(four)]

    near = lax.all_to_all(kv, Y, split_axis=0, concat_axis=0, tiled=True)
    far = swap(near)

    scratch = [vmem(8 * block, 256), vmem(8 * block, VDIM)]
    partial, stats, padded = kernel_call(
        attention_near_body,
        limit=12,
        out_shape=(
            jax.ShapeDtypeStruct((4, block, VDIM), jnp.float32),
            jax.ShapeDtypeStruct((4, block, 2 * VDIM), jnp.float32),
            jax.ShapeDtypeStruct((4, block, 256), jnp.bfloat16),
        ),
        in_specs=[VM] * 2,
        out_specs=(VM, VM, VM),
        scratch_shapes=scratch,
    )(queries, near)
    attended = kernel_call(
        attention_far_body,
        limit=12,
        out_shape=jax.ShapeDtypeStruct((4, block, VDIM), jnp.bfloat16),
        in_specs=[SM] + [VM] * 4,
        out_specs=VM,
        scratch_shapes=scratch,
    )(at, padded, far, partial, stats)
    attended = attended.reshape(4 * tp_size, block // tp_size, VDIM)
    attended = lax.all_to_all(attended, ("quad", "tp"), split_axis=0, concat_axis=0, tiled=True)

    stream, outgoing = kernel_call(
        project_body,
        limit=10,
        out_shape=(
            jax.ShapeDtypeStruct((rows, D), jnp.bfloat16),
            jax.ShapeDtypeStruct((2048, LANE), jnp.bfloat16),
        ),
        in_specs=[SM] + [VM] * 12,
        out_specs=(VM, VM),
        scratch_shapes=[vmem(256, D)],
    )(at, attended, *weights, res, norm_gain.reshape(1, D), meta)

    def exchange(x):
        x = x.reshape(128, 16, LANE)
        return lax.all_to_all(x, ALL, split_axis=0, concat_axis=0, tiled=True).reshape(2048, LANE)

    arrived = exchange(outgoing)
    served = kernel_call(
        expert_body,
        limit=10,
        out_shape=jax.ShapeDtypeStruct((2048, LANE), jnp.bfloat16),
        in_specs=[VM] * 4,
        out_specs=VM,
        scratch_shapes=[vmem(256, D)],
    )(arrived, w_gate[0], w_up[0], w_down[0])
    returned = exchange(served)
    combined = kernel_call(
        combine_body,
        limit=8,
        out_shape=jax.ShapeDtypeStruct(residual.shape, jnp.bfloat16),
        in_specs=[VM] * 3,
        out_specs=VM,
        scratch_shapes=[vmem(256, D)],
    )(returned, stream, meta)
    return combined


def solution(mesh):
    shape = mesh.shape
    devices = np.asarray(mesh.devices).reshape(
        shape["grp"], 2, 4, shape["sp"] // 8, shape["tp"]
    )
    fine = Mesh(devices, ("grp", "half", "quad", "core", "tp"))
    sp = ("half", "quad", "core")
    both = ("half", "quad", "core", "tp")
    placed = (
        P(both, "grp", None),
        P(sp, "grp", "tp"),
        P(sp, "grp", None),
        P(sp, "grp", None),
        P(),
        P(None, "tp"),
        P(None, "tp"),
        P("tp", None),
        P(),
        P(both, "grp"),
        P(both, "grp", None),
        P(both, "grp", None),
        P(both, None, None),
        P(both, None, None),
        P(both, None, None),
    )
    return jax.shard_map(
        layer, mesh=fine, in_specs=placed, out_specs=P(both, "grp", None), check_vma=False
    )
```
